32 devices in a mesh: tp: 32 (over z, y, x, core).
Axes of the slice: x: 2, y: 2, z: 4, core: 2. Of those that a mesh axis runs over, the one named last changes fastest.
Arguments:
- stream: bfloat16 [1024, 2048], P('tp'), may hold values from -15 to 15
- norm_gain: bfloat16 [4096], replicated, may hold values from 0.099609375 to 1.8984375
- query_weight: bfloat16 [65536, 128], P('tp'), may hold values from -0.09375 to 0.09375
- key_weight: bfloat16 [65536, 128], P('tp'), may hold values from -0.09375 to 0.09375
- value_weight: bfloat16 [65536, 128], P('tp'), may hold values from -0.09375 to 0.09375
- gate_weight: bfloat16 [65536, 128], P('tp'), may hold values from -0.09375 to 0.09375
- write_weight: bfloat16 [4096, 16], replicated, may hold values from -0.09375 to 0.09375
- decay_weight: bfloat16 [4096, 16], replicated, may hold values from -0.09375 to 0.09375
- decay_rate: float32 [16], replicated, may hold values from 0.02 to 2
- head_gain: bfloat16 [128], replicated, may hold values from 0.099609375 to 1.8984375
- out_weight: bfloat16 [65536, 128], P('tp'), may hold values from -0.125 to 0.125
- state: float32 [8192, 128, 128], P('tp'), may hold values from -4 to 4
Outputs:
- stream_out: bfloat16 [1024, 2048], P('tp')
- state_out: float32 [8192, 128, 128], P('tp')
The draws below stay inside these ranges and needn't reach their ends.
All inputs are finite; a program needn't handle non-finite values.
Results may differ from the reference program's by a relative error of at most 0.012.
Values may be sent and summed in bfloat16 or wider, within the bound.
A program may use at most 128 MiB of HBM per device.

```python
import math
import jax
import jax.numpy as jnp
from jax import lax

D = 4096
H = 16
DK = 128
BATCH = 512
SEQ_GROUPS = 2
DG = 2048
BG = 256


def draw_stream(key, part):
    key_vals, key_scales = jax.random.split(jax.random.fold_in(key, 17))
    values = jnp.clip(jax.random.normal(key_vals, (BATCH, D), jnp.float32), -5.0, 5.0)
    scales = jnp.exp(jax.random.uniform(key_scales, (D // 128,), jnp.float32, jnp.log(0.3), jnp.log(3.0)))
    whole = values * jnp.repeat(scales, 128)[None, :]
    return whole.reshape(BATCH, SEQ_GROUPS, DG).transpose(1, 0, 2).reshape(SEQ_GROUPS * BATCH, DG).astype(jnp.bfloat16)


def level_of(stream_key, shape, pieces, smallest, top_value):
    loudness, own = 1.0, jax.random.fold_in(stream_key, 6)
    for dim, parts in pieces:
        draws = jnp.exp(jax.random.uniform(jax.random.fold_in(own, dim), (parts,), jnp.float32, smallest / len(pieces), top_value / len(pieces)))
        loudness = loudness * jnp.repeat(draws, shape[dim] // parts).reshape([-1 if axis == dim else 1 for axis in range(len(shape))])
    return loudness


def noise(stream_key, shape, spread, bound, cuts=(), dtype=jnp.bfloat16):
    values = spread * jax.random.normal(stream_key, shape, jnp.float32)
    if cuts:
        values = values * level_of(stream_key, shape, cuts, -0.22, 0.18)
    return jnp.clip(values, -bound, bound).astype(dtype)


def setup_inputs(seed: int = 0) -> dict:
    key_list = jax.random.split(jax.random.key(seed), 13)
    return {
        "stream": draw_stream(jax.random.fold_in(key_list[12], 71), 0),
        "norm_gain": jnp.clip(1.0 + 0.18 * jax.random.normal(key_list[1], (D,), jnp.float32), 0.099609375, 1.8984375).astype(jnp.bfloat16),
        "query_weight": noise(key_list[2], (H * D, DK), D ** -0.5, 0.09375, ((0, 32),)),
        "key_weight": noise(key_list[3], (H * D, DK), D ** -0.5, 0.09375, ((0, 32),)),
        "value_weight": noise(key_list[4], (H * D, DK), D ** -0.5, 0.09375, ((0, 32),)),
        "gate_weight": noise(key_list[5], (H * D, DK), D ** -0.5, 0.09375, ((0, 32),)),
        "write_weight": noise(key_list[6], (D, H), D ** -0.5, 0.09375),
        "decay_weight": noise(key_list[7], (D, H), D ** -0.5, 0.09375),
        "decay_rate": jnp.clip(jnp.exp(jax.random.uniform(key_list[8], (H,), jnp.float32, math.log(0.02), math.log(2.0))), 0.02, 2.0),
        "head_gain": jnp.clip(1.0 + 0.18 * jax.random.normal(key_list[9], (DK,), jnp.float32), 0.099609375, 1.8984375).astype(jnp.bfloat16),
        "out_weight": noise(key_list[10], (H * D, DK), (H * DK) ** -0.5, 0.125, ((0, 32),)),
        "state": noise(key_list[11], (BATCH * H, DK, DK), 0.5, 4.0, ((0, 32),), jnp.float32),
    }


EPS = 1e-06

def reference(stream, norm_gain, query_weight, key_weight, value_weight, gate_weight, write_weight, decay_weight, decay_rate, head_gain, out_weight, state):
    highest = lax.Precision.HIGHEST
    stream_f = stream.reshape(SEQ_GROUPS, BATCH, DG).transpose(1, 0, 2).reshape(BATCH, D).astype(jnp.float32)
    gained = (stream_f * norm_gain.astype(jnp.float32)).astype(jnp.bfloat16)
    row_scale = lax.rsqrt(lax.optimization_barrier(jnp.mean(stream_f * stream_f, axis=-1)) + EPS)

    def logical(weight):
        return weight.reshape(SEQ_GROUPS, H, DG, DK).transpose(0, 2, 1, 3).reshape(D, H * DK)

    def project(weight):
        product = jnp.dot(gained, weight, preferred_element_type=jnp.float32)
        return (product * row_scale[:, None]).astype(jnp.bfloat16).astype(jnp.float32)
    query_raw = project(logical(query_weight)).reshape(BATCH, H, DK)
    key_raw = project(logical(key_weight)).reshape(BATCH, H, DK)
    value_vec = project(logical(value_weight)).reshape(BATCH, H, DK)
    gate_vec = project(logical(gate_weight)).reshape(BATCH, H, DK)
    write_pre = project(write_weight)
    decay_pre = project(decay_weight)
    query_vec = query_raw * lax.rsqrt(lax.optimization_barrier(jnp.sum(query_raw * query_raw, axis=-1, keepdims=True)) + EPS) * DK ** (-0.5)
    key_vec = key_raw * lax.rsqrt(lax.optimization_barrier(jnp.sum(key_raw * key_raw, axis=-1, keepdims=True)) + EPS)
    strength = jax.nn.sigmoid(write_pre)
    decay_factor = jnp.exp(-decay_rate[None, :] * jax.nn.softplus(decay_pre))
    memory = state.reshape(SEQ_GROUPS, H, BG, DK, DK).transpose(0, 2, 1, 3, 4).reshape(BATCH, H, DK, DK)
    recalled = jnp.einsum('bhdj,bhd->bhj', memory, key_vec, precision=highest)
    correction = strength[..., None] * (value_vec - decay_factor[..., None] * recalled)
    updated = decay_factor[..., None, None] * memory + key_vec[..., :, None] * correction[..., None, :]
    readout = jnp.einsum('bhdj,bhd->bhj', updated, query_vec, precision=highest)
    scaling = lax.rsqrt(lax.optimization_barrier(jnp.mean(readout * readout, axis=-1)) + EPS)
    gated_rows = (readout * head_gain.astype(jnp.float32) * jax.nn.silu(gate_vec)).astype(jnp.bfloat16)
    out_heads = out_weight.reshape(SEQ_GROUPS, H, DG, DK).transpose(1, 3, 0, 2).reshape(H, DK, D)
    head_sums = jnp.zeros((BATCH, D), jnp.float32)
    for head_index in range(H):
        term = jnp.dot(gated_rows[:, head_index], out_heads[head_index], preferred_element_type=jnp.float32)
        head_sums = head_sums + term * scaling[:, head_index, None]
    result = (stream_f + head_sums).astype(jnp.bfloat16)
    stream_out = result.reshape(BATCH, SEQ_GROUPS, DG).transpose(1, 0, 2).reshape(SEQ_GROUPS * BATCH, DG)
    state_out = updated.reshape(SEQ_GROUPS, BG, H, DK, DK).transpose(0, 2, 1, 3, 4).reshape(BATCH * H, DK, DK)
    return (stream_out, state_out)
```

```python
import jax
import jax.numpy as jnp
from jax import lax
from jax.experimental import pallas as pl
from jax.experimental.pallas import tpu as pltpu
from jax.sharding import PartitionSpec as P

EPS = 1e-06


def from_partner(shard, axis, bit):
    return lax.ppermute(shard, axis, [(i, i ^ 1 << bit) for i in range(lax.axis_size(axis))])


def shortened(shard):

    def short(part):
        return part.astype(jnp.bfloat16) if part.dtype == jnp.float32 else part

    return jax.tree.map(short, shard)


def state_kernel(state_ref, key_ref, query_ref, value_ref, rows_ref, new_ref, read_ref):
    count = state_ref.shape[0]
    for b in range(count):
        memory = state_ref[b]
        key = jnp.broadcast_to(key_ref[0, :, b : b + 1], memory.shape)
        query = jnp.broadcast_to(query_ref[0, :, b : b + 1], memory.shape)
        recalled = jnp.sum(memory * key, axis=0, keepdims=True)
        asked = jnp.sum(memory * query, axis=0, keepdims=True)
        strength = rows_ref[0, b : b + 1, :]
        factor = rows_ref[1, b : b + 1, :]
        overlap = rows_ref[2, b : b + 1, :]
        change = strength * (value_ref[b : b + 1, :] - factor * recalled)
        read_ref[b : b + 1, :] = factor * asked + overlap * change
        new_ref[b] = factor * memory + key * change


def state_step(state, query, key, value, strength, factor):
    count, size, _ = state.shape
    block = min(16, count)
    steps = count // block
    overlap = jnp.sum(query * key, axis=1)
    rows = jnp.stack(
        [jnp.broadcast_to(m[:, None], (count, size)) for m in (strength, factor, overlap)]
    )

    def columns(vec):
        return vec.reshape(steps, block, size).transpose(0, 2, 1)

    return pl.pallas_call(
        state_kernel,
        grid=(steps,),
        in_specs=[
            pl.BlockSpec((block, size, size), lambda i: (i, 0, 0)),
            pl.BlockSpec((1, size, block), lambda i: (i, 0, 0)),
            pl.BlockSpec((1, size, block), lambda i: (i, 0, 0)),
            pl.BlockSpec((block, size), lambda i: (i, 0)),
            pl.BlockSpec((3, block, size), lambda i: (0, i, 0)),
        ],
        out_specs=[
            pl.BlockSpec((block, size, size), lambda i: (i, 0, 0)),
            pl.BlockSpec((block, size), lambda i: (i, 0)),
        ],
        out_shape=[
            jax.ShapeDtypeStruct(state.shape, state.dtype),
            jax.ShapeDtypeStruct((count, size), jnp.float32),
        ],
    )(state, columns(key), columns(query), value, rows)


def per_device(
    stream,
    norm_gain,
    query_weight,
    key_weight,
    value_weight,
    gate_weight,
    write_weight,
    decay_weight,
    decay_rate,
    head_gain,
    out_weight,
    state,
):
    devices = lax.axis_size("tp")
    my_index = lax.axis_index("tp")
    head_count = decay_rate.shape[0]
    head_size = head_gain.shape[0]
    group_count = devices // head_count
    head_bits = head_count.bit_length() - 1
    group_bits = group_count.bit_length() - 1
    my_head = my_index % head_count
    my_group = my_index // head_count
    own_rows, own_cols = stream.shape
    model_width = own_cols * group_count
    gathered = stream
    for bit_level in range(head_bits):
        partner = from_partner(gathered, "tp", bit_level)
        upper_bit = my_index // (1 << bit_level) % 2
        gathered = jnp.where(
            upper_bit == 1,
            jnp.concatenate([partner, gathered], 0),
            jnp.concatenate([gathered, partner], 0),
        )
    stream_f = gathered.astype(jnp.float32)
    gain_block = lax.dynamic_slice_in_dim(norm_gain, my_group * own_cols, own_cols, 0).astype(
        jnp.float32
    )
    gained = (stream_f * gain_block[None, :]).astype(jnp.bfloat16)
    squares = jnp.sum(stream_f * stream_f, axis=1)
    write_rows = lax.dynamic_slice(write_weight, (my_group * own_cols, my_head), (own_cols, 1))
    decay_rows = lax.dynamic_slice(decay_weight, (my_group * own_cols, my_head), (own_cols, 1))
    big_weights = jnp.concatenate([query_weight, key_weight, value_weight, gate_weight], axis=1)
    partial_value = jnp.dot(gained, big_weights, preferred_element_type=jnp.float32)
    small_part = jnp.dot(
        gained,
        jnp.concatenate([write_rows, decay_rows], axis=1),
        preferred_element_type=jnp.float32,
    )
    for step_index in range(group_bits):
        bit_level = head_bits + group_bits - 1 - step_index
        upper_bit = my_index // (1 << bit_level) % 2
        half_rows = partial_value.shape[0] // 2
        kept = [
            lax.dynamic_slice_in_dim(member, upper_bit * half_rows, half_rows, 0)
            for member in (partial_value, small_part, squares)
        ]
        sent = [
            lax.dynamic_slice_in_dim(member, (1 - upper_bit) * half_rows, half_rows, 0)
            for member in (partial_value, small_part, squares)
        ]
        received = from_partner(
            (shortened(sent[0]), shortened(sent[1]), shortened(sent[2])), "tp", bit_level
        )
        partial_value = kept[0] + received[0]
        small_part = kept[1] + received[1]
        squares = kept[2] + received[2]
    row_scale = lax.rsqrt(squares / model_width + EPS)
    projected = (partial_value * row_scale[:, None]).astype(jnp.bfloat16).astype(jnp.float32)
    small_pre = (small_part * row_scale[:, None]).astype(jnp.bfloat16).astype(jnp.float32)
    query_raw = projected[:, :head_size]
    key_raw = projected[:, head_size : 2 * head_size]
    value_vec = projected[:, 2 * head_size : 3 * head_size]
    gate_vec = projected[:, 3 * head_size :]
    query_vec = (
        query_raw
        * lax.rsqrt(jnp.sum(query_raw * query_raw, axis=-1, keepdims=True) + EPS)
        * head_size ** (-0.5)
    )
    key_vec = key_raw * lax.rsqrt(jnp.sum(key_raw * key_raw, axis=-1, keepdims=True) + EPS)
    strength = jax.nn.sigmoid(small_pre[:, 0])
    rate_value = lax.dynamic_slice_in_dim(decay_rate, my_head, 1, 0)[0]
    decay_factor = jnp.exp(-rate_value * jax.nn.softplus(small_pre[:, 1]))
    updated, readout = state_step(state, query_vec, key_vec, value_vec, strength, decay_factor)
    scaling = lax.rsqrt(jnp.mean(readout * readout, axis=1) + EPS)
    gated = (readout * head_gain.astype(jnp.float32)[None, :] * jax.nn.silu(gate_vec)).astype(
        jnp.bfloat16
    )
    all_gated = gated
    all_scaling = scaling
    for step_index in range(group_bits):
        bit_level = head_bits + step_index
        upper_bit = my_index // (1 << bit_level) % 2
        other_gated, other_scaling = (
            from_partner(all_gated, "tp", bit_level),
            from_partner(all_scaling.astype(jnp.bfloat16), "tp", bit_level).astype(
                all_scaling.dtype
            ),
        )
        all_gated = jnp.where(
            upper_bit == 1,
            jnp.concatenate([other_gated, all_gated], 0),
            jnp.concatenate([all_gated, other_gated], 0),
        )
        all_scaling = jnp.where(
            upper_bit == 1,
            jnp.concatenate([other_scaling, all_scaling], 0),
            jnp.concatenate([all_scaling, other_scaling], 0),
        )
    head_sums = (
        lax.dot_general(
            all_gated, out_weight, (((1,), (1,)), ((), ())), preferred_element_type=jnp.float32
        )
        * all_scaling[:, None]
    )
    for step_index in range(head_bits):
        bit_level = head_bits - 1 - step_index
        upper_bit = my_index // (1 << bit_level) % 2
        half_rows = head_sums.shape[0] // 2
        kept_sums = lax.dynamic_slice_in_dim(head_sums, upper_bit * half_rows, half_rows, 0)
        sent_sums = lax.dynamic_slice_in_dim(head_sums, (1 - upper_bit) * half_rows, half_rows, 0)
        head_sums = kept_sums + from_partner(
            sent_sums.astype(jnp.bfloat16), "tp", bit_level
        ).astype(sent_sums.dtype)
    result = (stream.astype(jnp.float32) + head_sums).astype(jnp.bfloat16)
    return (result, updated)


def solution(mesh):
    placed = (
        P("tp", None),
        P(),
        P("tp", None),
        P("tp", None),
        P("tp", None),
        P("tp", None),
        P(),
        P(),
        P(),
        P(),
        P("tp", None),
        P("tp", None, None),
    )
    return jax.shard_map(
        per_device,
        mesh=mesh,
        in_specs=placed,
        out_specs=(P("tp", None), P("tp", None, None)),
        check_vma=False,
    )
```

```python
import functools

import jax
import jax.numpy as jnp
from jax import lax
from jax.experimental import pallas as pl
from jax.experimental.pallas import tpu as pltpu
from jax.sharding import PartitionSpec as P

EPS = 1e-06
MESH = pl.DeviceIdType.MESH
VMEM = pl.BlockSpec(memory_space=pltpu.VMEM)
SMALL = 16


def flip(me, bits):
    other = me
    for bit in bits:
        other = other + (1 - 2 * ((me // (1 << bit)) % 2)) * (1 << bit)
    return other


def parts_of(cols, dims):
    tiles = cols // 128
    count = max(1, min(dims, tiles))
    cuts = [tiles * i // count * 128 for i in range(count + 1)]
    ranges = [(cuts[i], cuts[i + 1] - cuts[i]) for i in range(count)]
    orders = [[1 + (i + j) % dims for j in range(dims)] for i in range(count)]
    return list(zip(ranges, orders))


def masks_of(order):
    sets = [((), -1)]
    for step in range(len(order)):
        sets = sets + [(bits + (order[step],), step) for bits, _ in sets]
    return sets


def key_of(bits):
    return sum(1 << (bit - 1) for bit in bits)


def enter(devices):
    barrier = pltpu.get_barrier_semaphore()
    for device in devices:
        pl.semaphore_signal(barrier, inc=1, device_id=(device,), device_id_type=MESH)
    pl.semaphore_wait(barrier, len(devices))


def remote(source, target, send_sem, recv_sem, device):
    return pltpu.make_async_remote_copy(
        src_ref=source,
        dst_ref=target,
        send_sem=send_sem,
        recv_sem=recv_sem,
        device_id=(device,),
        device_id_type=MESH,
    )


def project_kernel(
    heads,
    groups,
    stream_ref,
    gain_ref,
    query_w,
    key_w,
    value_w,
    gate_w,
    write_w,
    decay_w,
    rate_ref,
    query_out,
    key_out,
    value_out,
    gate_out,
    side_out,
    gathered,
    partial,
    sent,
    received,
    small_sent,
    small_received,
    turned,
    ici_send,
    ici_recv,
    core_send,
    core_recv,
    group_send,
    group_recv,
    small_send,
    small_recv,
):
    me = lax.axis_index("tp")
    place = me % heads
    group = me // heads
    rows, cols = stream_ref.shape
    batch = gathered.shape[0]
    group_rows = batch // groups
    dims = heads.bit_length() - 2
    sibling = flip(me, (0,))
    neighbours = [flip(me, (bit,)) for bit in range(1, dims + 1)]
    others = [place + heads * ((group + j) % groups) for j in range(1, groups)]
    enter([sibling] + neighbours + others)

    def block(device_place, part):
        (start, width), _ = part
        begin = pl.multiple_of(device_place * rows, rows)
        return gathered.at[pl.ds(begin, rows), pl.ds(start, width)]

    parts = parts_of(cols, dims)
    sends = []
    arrivals = []
    core_copies = []

    def pass_on(p, part, bits, step):
        order = part[1]
        origin = flip(place, bits)
        if bits:
            source = block(origin, part)
        else:
            source = stream_ref.at[:, pl.ds(part[0][0], part[0][1])]
        for later in range(step + 1, dims):
            landed = key_of(bits + (order[later],))
            copy = remote(
                source,
                block(origin, part),
                ici_send.at[p, landed],
                ici_recv.at[p, landed],
                flip(me, (order[later],)),
            )
            copy.start()
            sends.append(copy)
        own = key_of(bits)
        copy = remote(
            source, block(origin, part), core_send.at[p, own], core_recv.at[p, own], sibling
        )
        copy.start()
        core_copies.append(copy)

    def arrived(p, part, bits):
        landed = key_of(bits)
        target = block(flip(place, bits), part)
        remote(target, target, ici_send.at[p, landed], ici_recv.at[p, landed], sibling).wait_recv()

    for p, part in enumerate(parts):
        pass_on(p, part, (), -1)
    own_rows = pl.ds(pl.multiple_of(place * rows, rows), rows)
    gathered[own_rows, :] = stream_ref[...]
    for index in range(1, 1 << dims):
        for p, part in enumerate(parts):
            bits, step = masks_of(part[1])[index]
            arrived(p, part, bits)
            pass_on(p, part, bits, step)
    for copy in core_copies:
        copy.wait_recv()

    gain = gain_ref[group].astype(jnp.float32)
    write_block = write_w[group]
    decay_block = decay_w[group]
    size = query_w.shape[1]

    def project(begin, count, at):
        x = gathered[pl.ds(begin, count), :].astype(jnp.float32)
        gained = (x * gain).astype(jnp.bfloat16)
        for i, weight in enumerate((query_w, key_w, value_w, gate_w)):
            partial[pl.ds(at, count), i * size : (i + 1) * size] = jnp.dot(
                gained, weight[...], preferred_element_type=jnp.float32
            )
        mine = lax.broadcasted_iota(jnp.int32, (count, heads), 1) == place
        pre = [
            jnp.sum(
                jnp.where(mine, jnp.dot(gained, w, preferred_element_type=jnp.float32), 0.0),
                axis=1,
                keepdims=True,
            )
            for w in (write_block, decay_block)
        ]
        squares = jnp.sum(x * x, axis=1, keepdims=True)
        lane = lax.broadcasted_iota(jnp.int32, (count, 128), 1)
        return jnp.where(
            lane == 0, pre[0], jnp.where(lane == 1, pre[1], jnp.where(lane == 2, squares, 0.0))
        )

    copies = []
    wide = max(group_rows, 128)
    for j in list(range(1, groups)) + [0]:
        target_group = (group + j) % groups
        begin = pl.multiple_of(target_group * group_rows, group_rows)
        side = project(begin, group_rows, 0)
        if j:
            sent[j - 1] = partial[...].astype(jnp.bfloat16)
            turned[0:group_rows, :] = side
            flat = turned[...].T
            small_sent[j - 1] = flat[0:SMALL, 0:group_rows].astype(jnp.bfloat16)
            for source, target, send, recv in (
                (sent, received, group_send, group_recv),
                (small_sent, small_received, small_send, small_recv),
            ):
                copy = remote(
                    source.at[j - 1],
                    target.at[j - 1],
                    send.at[j - 1],
                    recv.at[j - 1],
                    others[j - 1],
                )
                copy.start()
                copies.append(copy)
    total = partial[...]
    turned[0:group_rows, :] = side
    flat = turned[...].T[0:SMALL, :]
    for copy in copies:
        copy.wait_recv()
    for j in range(1, groups):
        total = total + received[j - 1].astype(jnp.float32)
    small_total = flat[:, 0:group_rows]
    for j in range(1, groups):
        small_total = small_total + small_received[j - 1].astype(jnp.float32)
    turned_back = jnp.concatenate(
        [small_total, jnp.zeros((SMALL, wide - group_rows), jnp.float32)], axis=1
    ) if wide > group_rows else small_total
    side = jnp.concatenate(
        [turned_back, jnp.zeros((128 - SMALL, wide), jnp.float32)], axis=0
    ).T[0:group_rows]
    scale = lax.rsqrt(side[:, 2:3] / (cols * groups) + EPS)

    def rounded(v):
        return v.astype(jnp.bfloat16).astype(jnp.float32)

    projected = rounded(total * scale)
    query = projected[:, :size]
    key = projected[:, size : 2 * size]
    query = query * lax.rsqrt(jnp.sum(query * query, axis=1, keepdims=True) + EPS) * size**-0.5
    key = key * lax.rsqrt(jnp.sum(key * key, axis=1, keepdims=True) + EPS)
    query_out[...] = query
    key_out[...] = key
    value_out[...] = projected[:, 2 * size : 3 * size]
    gate_out[...] = projected[:, 3 * size :]
    pre = rounded(side * scale)
    strength = jax.nn.sigmoid(pre[:, 0:1])
    mine = lax.broadcasted_iota(jnp.int32, rate_ref.shape, 1) == place
    rate = jnp.sum(jnp.where(mine, rate_ref[...], 0.0), axis=1, keepdims=True)
    decay = pre[:, 1:2]
    softplus = jnp.maximum(decay, 0.0) + jnp.log(1.0 + jnp.exp(-jnp.abs(decay)))
    factor = jnp.exp(-rate * softplus)
    overlap = jnp.sum(query * key, axis=1, keepdims=True)
    side_out[0] = jnp.broadcast_to(strength, (group_rows, size))
    side_out[1] = jnp.broadcast_to(factor, (group_rows, size))
    side_out[2] = jnp.broadcast_to(overlap, (group_rows, size))
    for copy in sends + core_copies + copies:
        copy.wait_send()


def project(stream, norm_gain, weights, write_weight, decay_weight, rate, heads, groups):
    rows, cols = stream.shape
    batch = rows * heads
    group_rows = batch // groups
    size = weights[0].shape[1]
    dims = heads.bit_length() - 2
    parts = len(parts_of(cols, dims))
    extra = groups - 1
    dma = pltpu.SemaphoreType.DMA
    vec = jax.ShapeDtypeStruct((group_rows, size), jnp.float32)
    return pl.pallas_call(
        functools.partial(project_kernel, heads, groups),
        in_specs=[VMEM] * 9,
        out_specs=[VMEM] * 5,
        out_shape=[vec] * 4 + [jax.ShapeDtypeStruct((3, group_rows, size), jnp.float32)],
        scratch_shapes=[
            pltpu.VMEM((batch, cols), jnp.bfloat16),
            pltpu.VMEM((group_rows, 4 * size), jnp.float32),
            pltpu.VMEM((extra, group_rows, 4 * size), jnp.bfloat16),
            pltpu.VMEM((extra, group_rows, 4 * size), jnp.bfloat16),
            pltpu.VMEM((extra, SMALL, group_rows), jnp.bfloat16),
            pltpu.VMEM((extra, SMALL, group_rows), jnp.bfloat16),
            pltpu.VMEM((max(group_rows, 128), 128), jnp.float32),
            dma((parts, 1 << dims)),
            dma((parts, 1 << dims)),
            dma((parts, 1 << dims)),
            dma((parts, 1 << dims)),
            dma((extra,)),
            dma((extra,)),
            dma((extra,)),
            dma((extra,)),
        ],
        compiler_params=pltpu.CompilerParams(
            collective_id=0, has_side_effects=True, vmem_limit_bytes=48 * 1024 * 1024
        ),
    )(
        stream,
        norm_gain.reshape(groups, 1, cols),
        *weights,
        write_weight.reshape(groups, cols, heads),
        decay_weight.reshape(groups, cols, heads),
        rate.reshape(1, heads),
    )


def split(v):
    high = v.astype(jnp.bfloat16)
    return high, (v - high.astype(jnp.float32)).astype(jnp.bfloat16)


def state_kernel(state_ref, key_ref, query_ref, value_ref, side_ref, new_ref, read_ref):
    count, size, _ = state_ref.shape
    key_high, key_low = split(key_ref[...])
    query_high, query_low = split(query_ref[...])
    spots = lax.broadcasted_iota(jnp.int32, (count, size), 0)
    recalled = jnp.zeros((count, size), jnp.float32)
    asked = jnp.zeros((count, size), jnp.float32)
    four = jnp.concatenate([key_high, key_low, query_high, query_low], axis=0)
    for b in range(count):
        memory = state_ref[b].astype(jnp.bfloat16)
        both = jnp.dot(four, memory, preferred_element_type=jnp.float32)
        recalled = jnp.where(spots == b, both[0:count] + both[count : 2 * count], recalled)
        asked = jnp.where(
            spots == b, both[2 * count : 3 * count] + both[3 * count : 4 * count], asked
        )
    strength, factor, overlap = side_ref[0], side_ref[1], side_ref[2]
    change = strength * (value_ref[...] - factor * recalled)
    read_ref[...] = factor * asked + overlap * change
    change_high, change_low = split(change)
    left = jnp.concatenate([key_high, key_low, key_high], axis=0)
    right = jnp.concatenate([change_high, change_high, change_low], axis=0)
    wide_spots = lax.broadcasted_iota(jnp.int32, right.shape, 0) % count
    for b in range(count):
        only = jnp.where(wide_spots == b, right.astype(jnp.float32), 0.0).astype(jnp.bfloat16)
        outer = lax.dot_general(
            left, only, (((0,), (0,)), ((), ())), preferred_element_type=jnp.float32
        )
        new_ref[b] = factor[b : b + 1, :] * state_ref[b] + outer


def state_step(state, query, key, value, side):
    count, size, _ = state.shape
    block = min(16, count)
    row_spec = pl.BlockSpec((block, size), lambda i: (i, 0))
    return pl.pallas_call(
        state_kernel,
        grid=(count // block,),
        in_specs=[
            pl.BlockSpec((block, size, size), lambda i: (i, 0, 0)),
            row_spec,
            row_spec,
            row_spec,
            pl.BlockSpec((3, block, size), lambda i: (0, i, 0)),
        ],
        out_specs=[pl.BlockSpec((block, size, size), lambda i: (i, 0, 0)), row_spec],
        out_shape=[
            jax.ShapeDtypeStruct(state.shape, state.dtype),
            jax.ShapeDtypeStruct((count, size), jnp.float32),
        ],
    )(state, key, query, value, side)


def output_kernel(
    heads,
    groups,
    stream_ref,
    gated_ref,
    scaling_ref,
    weight_ref,
    out_ref,
    all_gated,
    all_scaling,
    columns,
    held,
    core_out,
    core_in,
    hop_out,
    hop_in,
    gated_send,
    gated_recv,
    scaling_send,
    scaling_recv,
    core_send,
    core_recv,
    hop_send,
    hop_recv,
):
    me = lax.axis_index("tp")
    place = me % heads
    group = me // heads
    rows, cols = stream_ref.shape
    batch = all_gated.shape[0]
    group_rows = batch // groups
    dims = heads.bit_length() - 2
    chips = 1 << dims
    sibling = flip(me, (0,))
    neighbours = [flip(me, (bit,)) for bit in range(1, dims + 1)]
    others = [place + heads * ((group + j) % groups) for j in range(1, groups)]
    enter([sibling] + neighbours + others)
    own_rows = pl.ds(pl.multiple_of(group * group_rows, group_rows), group_rows)
    copies = []
    arriving = []
    for j in range(1, groups):
        for source, target, send, recv in (
            (gated_ref, all_gated.at[own_rows], gated_send, gated_recv),
            (scaling_ref, all_scaling.at[group], scaling_send, scaling_recv),
        ):
            copy = remote(source, target, send.at[j - 1], recv.at[j - 1], others[j - 1])
            copy.start()
            copies.append(copy)
    all_gated[own_rows, :] = gated_ref[...]
    all_scaling[group] = scaling_ref[...]
    for copy in copies:
        copy.wait_recv()
    wide = max(group_rows, 128)
    for g in range(groups):
        flat = all_scaling[g].astype(jnp.float32)
        if wide > group_rows:
            flat = jnp.concatenate(
                [flat, jnp.zeros((SMALL, wide - group_rows), jnp.float32)], axis=1
            )
        flat = jnp.concatenate([flat, jnp.zeros((128 - SMALL, wide), jnp.float32)], axis=0)
        columns[g * group_rows : (g + 1) * group_rows, :] = flat.T[0:group_rows]

    def relative(owner, mask):
        bits = tuple(bit for bit in range(1, dims + 1) if mask >> (bit - 1) & 1)
        begin = flip(owner, bits) * rows
        return pl.ds(pl.multiple_of(begin, rows), rows)

    def head_rows(owner, masks):
        picks = [relative(owner, mask) for mask in masks]
        left = jnp.concatenate([all_gated[pick, :] for pick in picks], axis=0)
        scale = jnp.concatenate([columns[pick, 0:1] for pick in picks], axis=0)
        product = lax.dot_general(
            left, weight_ref[...], (((1,), (1,)), ((), ())), preferred_element_type=jnp.float32
        )
        return product * scale

    core_copies = [
        remote(
            core_out.at[mask], core_in.at[mask], core_send.at[mask], core_recv.at[mask], sibling
        )
        for mask in range(chips)
    ]
    batch_of = min(4, chips)
    sweep = list(range(chips - 1, -1, -1))
    for first in range(0, chips, batch_of):
        masks = sweep[first : first + batch_of]
        product = head_rows(flip(place, (0,)), masks).astype(jnp.bfloat16)
        for i, mask in enumerate(masks):
            core_out[mask] = product[i * rows : (i + 1) * rows]
            core_copies[mask].start()
    for first in range(0, chips, batch_of):
        masks = sweep[first : first + batch_of]
        product = head_rows(place, masks)
        for i, mask in enumerate(masks):
            held[mask] = product[i * rows : (i + 1) * rows]
    for mask in sweep:
        core_copies[mask].wait_recv()
        held[mask] += core_in[mask].astype(jnp.float32)

    parts = parts_of(cols, dims)
    hops = []
    for step in range(dims):
        started = []
        for p, ((start, width), order) in enumerate(parts):
            span = pl.ds(start, width)
            crossed = [1 << (bit - 1) for bit in order[:step]]
            now = 1 << (order[step] - 1)
            for mask in range(chips):
                if any(mask & c for c in crossed) or not mask & now:
                    continue
                landed = mask - now
                hop_out[step, landed, :, span] = held[mask, :, span].astype(jnp.bfloat16)
                copy = remote(
                    hop_out.at[step, landed, :, span],
                    hop_in.at[step, landed, :, span],
                    hop_send.at[step, p, landed],
                    hop_recv.at[step, p, landed],
                    neighbours[order[step] - 1],
                )
                copy.start()
                started.append((landed, span, copy))
        for landed, span, copy in started:
            copy.wait_recv()
            held[landed, :, span] += hop_in[step, landed, :, span].astype(jnp.float32)
            hops.append(copy)
    out_ref[...] = (stream_ref[...].astype(jnp.float32) + held[0]).astype(jnp.bfloat16)
    for copy in copies + core_copies + hops:
        copy.wait_send()


def output(stream, gated, scaling, out_weight, heads, groups):
    rows, cols = stream.shape
    batch = rows * heads
    group_rows, size = gated.shape
    dims = heads.bit_length() - 2
    chips = 1 << dims
    parts = len(parts_of(cols, dims))
    extra = groups - 1
    dma = pltpu.SemaphoreType.DMA
    flat = jnp.broadcast_to(scaling.astype(jnp.bfloat16)[None, :], (SMALL, group_rows))
    return pl.pallas_call(
        functools.partial(output_kernel, heads, groups),
        in_specs=[VMEM] * 4,
        out_specs=VMEM,
        out_shape=jax.ShapeDtypeStruct(stream.shape, stream.dtype),
        scratch_shapes=[
            pltpu.VMEM((batch, size), jnp.bfloat16),
            pltpu.VMEM((groups, SMALL, group_rows), jnp.bfloat16),
            pltpu.VMEM((batch, 128), jnp.float32),
            pltpu.VMEM((chips, rows, cols), jnp.float32),
            pltpu.VMEM((chips, rows, cols), jnp.bfloat16),
            pltpu.VMEM((chips, rows, cols), jnp.bfloat16),
            pltpu.VMEM((dims, chips, rows, cols), jnp.bfloat16),
            pltpu.VMEM((dims, chips, rows, cols), jnp.bfloat16),
            dma((extra,)),
            dma((extra,)),
            dma((extra,)),
            dma((extra,)),
            dma((chips,)),
            dma((chips,)),
            dma((dims, parts, chips)),
            dma((dims, parts, chips)),
        ],
        compiler_params=pltpu.CompilerParams(
            collective_id=1, has_side_effects=True, vmem_limit_bytes=48 * 1024 * 1024
        ),
    )(stream, gated, flat, out_weight)


def per_device(
    stream,
    norm_gain,
    query_weight,
    key_weight,
    value_weight,
    gate_weight,
    write_weight,
    decay_weight,
    decay_rate,
    head_gain,
    out_weight,
    state,
):
    heads = decay_rate.shape[0]
    groups = lax.axis_size("tp") // heads
    weights = (query_weight, key_weight, value_weight, gate_weight)
    query, key, value, gate, side = project(
        stream, norm_gain, weights, write_weight, decay_weight, decay_rate, heads, groups
    )
    updated, readout = state_step(state, query, key, value, side)
    scaling = lax.rsqrt(jnp.mean(readout * readout, axis=1) + EPS)
    gated = (readout * head_gain.astype(jnp.float32)[None, :] * jax.nn.silu(gate)).astype(
        jnp.bfloat16
    )
    result = output(stream, gated, scaling, out_weight, heads, groups)
    return (result, updated)


def solution(mesh):
    placed = (
        P("tp", None),
        P(),
        P("tp", None),
        P("tp", None),
        P("tp", None),
        P("tp", None),
        P(),
        P(),
        P(),
        P(),
        P("tp", None),
        P("tp", None, None),
    )
    return jax.shard_map(
        per_device,
        mesh=mesh,
        in_specs=placed,
        out_specs=(P("tp", None), P("tp", None, None)),
        check_vma=False,
    )
```

```python
import functools

import jax
import jax.numpy as jnp
from jax import lax
from jax.experimental import pallas as pl
from jax.experimental.pallas import tpu as pltpu
from jax.sharding import PartitionSpec as P

EPS = 1e-06
MESH = pl.DeviceIdType.MESH
VMEM = pl.BlockSpec(memory_space=pltpu.VMEM)
SMALL = 16


def flip(me, bits):
    other = me
    for bit in bits:
        other = other + (1 - 2 * ((me // (1 << bit)) % 2)) * (1 << bit)
    return other


def parts_of(cols, dims):
    tiles = cols // 128
    count = max(1, min(dims, tiles))
    cuts = [tiles * i // count * 128 for i in range(count + 1)]
    ranges = [(cuts[i], cuts[i + 1] - cuts[i]) for i in range(count)]
    orders = [[1 + (i + j) % dims for j in range(dims)] for i in range(count)]
    return list(zip(ranges, orders))


def masks_of(order):
    sets = [((), -1)]
    for step in range(len(order)):
        sets = sets + [(bits + (order[step],), step) for bits, _ in sets]
    return sets


def key_of(bits):
    return sum(1 << (bit - 1) for bit in bits)


def enter(devices):
    barrier = pltpu.get_barrier_semaphore()
    for device in devices:
        pl.semaphore_signal(barrier, inc=1, device_id=(device,), device_id_type=MESH)
    pl.semaphore_wait(barrier, len(devices))


def remote(source, target, send_sem, recv_sem, device):
    return pltpu.make_async_remote_copy(
        src_ref=source,
        dst_ref=target,
        send_sem=send_sem,
        recv_sem=recv_sem,
        device_id=(device,),
        device_id_type=MESH,
    )


def project_kernel(
    heads,
    groups,
    stream_ref,
    gain_ref,
    query_w,
    key_w,
    value_w,
    gate_w,
    write_w,
    decay_w,
    rate_ref,
    packed_out,
    gathered,
    weights,
    write_t,
    decay_t,
    local_sems,
    partial,
    sent,
    received,
    small_sent,
    small_received,
    turned,
    ici_send,
    ici_recv,
    core_send,
    core_recv,
    group_send,
    group_recv,
    small_send,
    small_recv,
):
    me = lax.axis_index("tp")
    place = me % heads
    group = me // heads
    rows, cols = stream_ref.shape
    batch = gathered.shape[0]
    group_rows = batch // groups
    dims = heads.bit_length() - 2
    sibling = flip(me, (0,))
    neighbours = [flip(me, (bit,)) for bit in range(1, dims + 1)]
    others = [place + heads * ((group + j) % groups) for j in range(1, groups)]
    size = query_w.shape[1]
    own_cols = pl.ds(pl.multiple_of(group * cols, cols), cols)
    fetches = [
        pltpu.make_async_copy(
            weight, weights.at[:, i * size : (i + 1) * size], local_sems.at[i]
        )
        for i, weight in enumerate((query_w, key_w, value_w, gate_w))
    ] + [
        pltpu.make_async_copy(source.at[:, own_cols], target, local_sems.at[4 + i])
        for i, (source, target) in enumerate(((write_w, write_t), (decay_w, decay_t)))
    ]
    for fetch in fetches:
        fetch.start()
    enter([sibling] + neighbours + others)

    def block(device_place, part):
        (start, width), _ = part
        begin = pl.multiple_of(device_place * rows, rows)
        return gathered.at[pl.ds(begin, rows), pl.ds(start, width)]

    parts = parts_of(cols, dims)
    sends = []
    arrivals = []
    core_copies = []

    def pass_on(p, part, bits, step):
        order = part[1]
        origin = flip(place, bits)
        if bits:
            source = block(origin, part)
        else:
            source = stream_ref.at[:, pl.ds(part[0][0], part[0][1])]
        for later in range(step + 1, dims):
            landed = key_of(bits + (order[later],))
            copy = remote(
                source,
                block(origin, part),
                ici_send.at[p, landed],
                ici_recv.at[p, landed],
                flip(me, (order[later],)),
            )
            copy.start()
            sends.append(copy)
        own = key_of(bits)
        copy = remote(
            source, block(origin, part), core_send.at[p, own], core_recv.at[p, own], sibling
        )
        copy.start()
        core_copies.append(copy)

    def arrived(p, part, bits):
        landed = key_of(bits)
        target = block(flip(place, bits), part)
        remote(target, target, ici_send.at[p, landed], ici_recv.at[p, landed], sibling).wait_recv()

    for p, part in enumerate(parts):
        pass_on(p, part, (), -1)
    own_rows = pl.ds(pl.multiple_of(place * rows, rows), rows)
    gathered[own_rows, :] = stream_ref[...]
    for index in range(1, 1 << dims):
        for p, part in enumerate(parts):
            bits, step = masks_of(part[1])[index]
            arrived(p, part, bits)
            pass_on(p, part, bits, step)
    for copy in core_copies:
        copy.wait_recv()

    gain = gain_ref[group].astype(jnp.float32)
    for fetch in fetches:
        fetch.wait()

    def project(begin, count, at):
        x = gathered[pl.ds(begin, count), :].astype(jnp.float32)
        gained = (x * gain).astype(jnp.bfloat16)
        partial[pl.ds(at, count), :] = jnp.dot(
            gained, weights[...], preferred_element_type=jnp.float32
        )
        mine = lax.broadcasted_iota(jnp.int32, (count, heads), 1) == place
        pre = [
            jnp.sum(
                jnp.where(
                    mine,
                    lax.dot_general(
                        gained,
                        w[...],
                        (((1,), (1,)), ((), ())),
                        preferred_element_type=jnp.float32,
                    ),
                    0.0,
                ),
                axis=1,
                keepdims=True,
            )
            for w in (write_t, decay_t)
        ]
        squares = jnp.sum(x * x, axis=1, keepdims=True)
        lane = lax.broadcasted_iota(jnp.int32, (count, 128), 1)
        return jnp.where(
            lane == 0, pre[0], jnp.where(lane == 1, pre[1], jnp.where(lane == 2, squares, 0.0))
        )

    copies = []
    wide = max(group_rows, 128)
    for j in list(range(1, groups)) + [0]:
        target_group = (group + j) % groups
        begin = pl.multiple_of(target_group * group_rows, group_rows)
        side = project(begin, group_rows, 0)
        if j:
            sent[j - 1] = partial[...].astype(jnp.bfloat16)
            turned[0:group_rows, :] = side
            flat = turned[...].T
            small_sent[j - 1] = flat[0:SMALL, 0:group_rows].astype(jnp.bfloat16)
            for source, target, send, recv in (
                (sent, received, group_send, group_recv),
                (small_sent, small_received, small_send, small_recv),
            ):
                copy = remote(
                    source.at[j - 1],
                    target.at[j - 1],
                    send.at[j - 1],
                    recv.at[j - 1],
                    others[j - 1],
                )
                copy.start()
                copies.append(copy)
    total = partial[...]
    turned[0:group_rows, :] = side
    flat = turned[...].T[0:SMALL, :]
    for copy in copies:
        copy.wait_recv()
    for j in range(1, groups):
        total = total + received[j - 1].astype(jnp.float32)
    small_total = flat[:, 0:group_rows]
    for j in range(1, groups):
        small_total = small_total + small_received[j - 1].astype(jnp.float32)
    turned_back = jnp.concatenate(
        [small_total, jnp.zeros((SMALL, wide - group_rows), jnp.float32)], axis=1
    ) if wide > group_rows else small_total
    side = jnp.concatenate(
        [turned_back, jnp.zeros((128 - SMALL, wide), jnp.float32)], axis=0
    ).T[0:group_rows]
    scale = lax.rsqrt(side[:, 2:3] / (cols * groups) + EPS)

    def rounded(v):
        return v.astype(jnp.bfloat16).astype(jnp.float32)

    projected = rounded(total * scale)
    query = projected[:, :size]
    key = projected[:, size : 2 * size]
    query = query * lax.rsqrt(jnp.sum(query * query, axis=1, keepdims=True) + EPS) * size**-0.5
    key = key * lax.rsqrt(jnp.sum(key * key, axis=1, keepdims=True) + EPS)
    packed_out[:, 3 * size : 4 * size] = query
    packed_out[:, 4 * size : 5 * size] = key
    packed_out[:, 5 * size :] = projected[:, 2 * size :]
    pre = rounded(side * scale)
    strength = jax.nn.sigmoid(pre[:, 0:1])
    mine = lax.broadcasted_iota(jnp.int32, rate_ref.shape, 1) == place
    rate = jnp.sum(jnp.where(mine, rate_ref[...], 0.0), axis=1, keepdims=True)
    decay = pre[:, 1:2]
    softplus = jnp.maximum(decay, 0.0) + jnp.log(1.0 + jnp.exp(-jnp.abs(decay)))
    factor = jnp.exp(-rate * softplus)
    overlap = jnp.sum(query * key, axis=1, keepdims=True)
    packed_out[:, 0 * size : 1 * size] = jnp.broadcast_to(strength, (group_rows, size))
    packed_out[:, 1 * size : 2 * size] = jnp.broadcast_to(factor, (group_rows, size))
    packed_out[:, 2 * size : 3 * size] = jnp.broadcast_to(overlap, (group_rows, size))
    for copy in sends + core_copies + copies:
        copy.wait_send()


def project(stream, norm_gain, weights, write_weight, decay_weight, rate, heads, groups):
    rows, cols = stream.shape
    batch = rows * heads
    group_rows = batch // groups
    size = weights[0].shape[1]
    dims = heads.bit_length() - 2
    parts = len(parts_of(cols, dims))
    extra = groups - 1
    dma = pltpu.SemaphoreType.DMA
    anywhere = pl.BlockSpec(memory_space=pl.ANY)
    return pl.pallas_call(
        functools.partial(project_kernel, heads, groups),
        in_specs=[VMEM] * 2 + [anywhere] * 6 + [VMEM],
        out_specs=VMEM,
        out_shape=jax.ShapeDtypeStruct((group_rows, 7 * size), jnp.float32),
        scratch_shapes=[
            pltpu.VMEM((batch, cols), jnp.bfloat16),
            pltpu.VMEM((cols, 4 * size), jnp.bfloat16),
            pltpu.VMEM((heads, cols), jnp.bfloat16),
            pltpu.VMEM((heads, cols), jnp.bfloat16),
            dma((6,)),
            pltpu.VMEM((group_rows, 4 * size), jnp.float32),
            pltpu.VMEM((extra, group_rows, 4 * size), jnp.bfloat16),
            pltpu.VMEM((extra, group_rows, 4 * size), jnp.bfloat16),
            pltpu.VMEM((extra, SMALL, group_rows), jnp.bfloat16),
            pltpu.VMEM((extra, SMALL, group_rows), jnp.bfloat16),
            pltpu.VMEM((max(group_rows, 128), 128), jnp.float32),
            dma((parts, 1 << dims)),
            dma((parts, 1 << dims)),
            dma((parts, 1 << dims)),
            dma((parts, 1 << dims)),
            dma((extra,)),
            dma((extra,)),
            dma((extra,)),
            dma((extra,)),
        ],
        compiler_params=pltpu.CompilerParams(
            collective_id=0, has_side_effects=True, vmem_limit_bytes=48 * 1024 * 1024
        ),
    )(
        stream,
        norm_gain.reshape(groups, 1, cols),
        *weights,
        write_weight.T,
        decay_weight.T,
        rate.reshape(1, heads),
    )


def split(v):
    high = v.astype(jnp.bfloat16)
    return high, (v - high.astype(jnp.float32)).astype(jnp.bfloat16)


def state_kernel(state_ref, key_ref, query_ref, value_ref, side_ref, new_ref, read_ref):
    count, size, _ = state_ref.shape
    key_high, key_low = split(key_ref[...])
    query_high, query_low = split(query_ref[...])
    four = jnp.concatenate([key_high, key_low, query_high, query_low], axis=0)
    spots = lax.broadcasted_iota(jnp.int32, four.shape, 0) % count

    def diagonal(rows):
        marks = spots[0 : rows.shape[0]]
        return jnp.concatenate(
            [jnp.where(marks == b, rows, jnp.zeros_like(rows)) for b in range(count)], axis=1
        )

    memory = state_ref[...].reshape(count * size, size).astype(jnp.bfloat16)
    both = jnp.dot(diagonal(four), memory, preferred_element_type=jnp.float32)
    recalled = both[0:count] + both[count : 2 * count]
    asked = both[2 * count : 3 * count] + both[3 * count : 4 * count]
    strength, factor, overlap = side_ref[:, 0:size], side_ref[:, size : 2 * size], side_ref[:, 2 * size :]
    change = strength * (value_ref[...] - factor * recalled)
    read_ref[...] = factor * asked + overlap * change
    change_high, change_low = split(change)
    left = jnp.concatenate([key_high, key_low, key_high], axis=0)
    left = jnp.concatenate([left, jnp.zeros((size - 3 * count, size), left.dtype)], axis=0)
    left = left.astype(jnp.float32).T.astype(jnp.bfloat16)[:, 0 : 3 * count]
    right = diagonal(jnp.concatenate([change_high, change_high, change_low], axis=0))
    outer = jnp.dot(left, right, preferred_element_type=jnp.float32)
    for b in range(count):
        new_ref[b] = factor[b : b + 1, :] * state_ref[b] + outer[:, b * size : (b + 1) * size]


def state_step(state, packed):
    count, size, _ = state.shape
    block = min(16, count)

    def columns(first, width):
        return pl.BlockSpec((block, width), lambda i: (i, first))

    return pl.pallas_call(
        state_kernel,
        grid=(count // block,),
        in_specs=[
            pl.BlockSpec((block, size, size), lambda i: (i, 0, 0)),
            columns(4, size),
            columns(3, size),
            columns(5, size),
            columns(0, 3 * size),
        ],
        out_specs=[pl.BlockSpec((block, size, size), lambda i: (i, 0, 0)), columns(0, size)],
        out_shape=[
            jax.ShapeDtypeStruct(state.shape, state.dtype),
            jax.ShapeDtypeStruct((count, size), jnp.float32),
        ],
    )(state, packed, packed, packed, packed)


def output_kernel(
    heads,
    groups,
    stream_ref,
    gated_ref,
    scaling_ref,
    weight_ref,
    out_ref,
    all_gated,
    all_scaling,
    columns,
    held,
    core_out,
    core_in,
    hop_out,
    hop_in,
    gated_send,
    gated_recv,
    scaling_send,
    scaling_recv,
    core_send,
    core_recv,
    hop_send,
    hop_recv,
):
    me = lax.axis_index("tp")
    place = me % heads
    group = me // heads
    rows, cols = stream_ref.shape
    batch = all_gated.shape[0]
    group_rows = batch // groups
    dims = heads.bit_length() - 2
    chips = 1 << dims
    sibling = flip(me, (0,))
    neighbours = [flip(me, (bit,)) for bit in range(1, dims + 1)]
    others = [place + heads * ((group + j) % groups) for j in range(1, groups)]
    enter([sibling] + neighbours + others)
    own_rows = pl.ds(pl.multiple_of(group * group_rows, group_rows), group_rows)
    copies = []
    arriving = []
    for j in range(1, groups):
        for source, target, send, recv in (
            (gated_ref, all_gated.at[own_rows], gated_send, gated_recv),
            (scaling_ref, all_scaling.at[group], scaling_send, scaling_recv),
        ):
            copy = remote(source, target, send.at[j - 1], recv.at[j - 1], others[j - 1])
            copy.start()
            copies.append(copy)
    all_gated[own_rows, :] = gated_ref[...]
    all_scaling[group] = scaling_ref[...]
    for copy in copies:
        copy.wait_recv()
    wide = max(group_rows, 128)
    for g in range(groups):
        flat = all_scaling[g].astype(jnp.float32)
        if wide > group_rows:
            flat = jnp.concatenate(
                [flat, jnp.zeros((SMALL, wide - group_rows), jnp.float32)], axis=1
            )
        flat = jnp.concatenate([flat, jnp.zeros((128 - SMALL, wide), jnp.float32)], axis=0)
        columns[g * group_rows : (g + 1) * group_rows, :] = flat.T[0:group_rows]

    def relative(owner, mask):
        bits = tuple(bit for bit in range(1, dims + 1) if mask >> (bit - 1) & 1)
        begin = flip(owner, bits) * rows
        return pl.ds(pl.multiple_of(begin, rows), rows)

    def head_rows(owner, masks):
        picks = [relative(owner, mask) for mask in masks]
        left = jnp.concatenate([all_gated[pick, :] for pick in picks], axis=0)
        scale = jnp.concatenate([columns[pick, 0:1] for pick in picks], axis=0)
        product = lax.dot_general(
            left, weight_ref[...], (((1,), (1,)), ((), ())), preferred_element_type=jnp.float32
        )
        return product * scale

    core_copies = [
        remote(
            core_out.at[mask], core_in.at[mask], core_send.at[mask], core_recv.at[mask], sibling
        )
        for mask in range(chips)
    ]
    batch_of = min(4, chips)
    sweep = list(range(chips - 1, -1, -1))
    for first in range(0, chips, batch_of):
        masks = sweep[first : first + batch_of]
        product = head_rows(flip(place, (0,)), masks).astype(jnp.bfloat16)
        for i, mask in enumerate(masks):
            core_out[mask] = product[i * rows : (i + 1) * rows]
            core_copies[mask].start()
    for first in range(0, chips, batch_of):
        masks = sweep[first : first + batch_of]
        product = head_rows(place, masks)
        for i, mask in enumerate(masks):
            held[mask] = product[i * rows : (i + 1) * rows]
    for mask in sweep:
        core_copies[mask].wait_recv()
        held[mask] += core_in[mask].astype(jnp.float32)

    parts = parts_of(cols, dims)
    hops = []
    for step in range(dims):
        started = []
        for p, ((start, width), order) in enumerate(parts):
            span = pl.ds(start, width)
            crossed = [1 << (bit - 1) for bit in order[:step]]
            now = 1 << (order[step] - 1)
            for mask in range(chips):
                if any(mask & c for c in crossed) or not mask & now:
                    continue
                landed = mask - now
                hop_out[step, landed, :, span] = held[mask, :, span].astype(jnp.bfloat16)
                copy = remote(
                    hop_out.at[step, landed, :, span],
                    hop_in.at[step, landed, :, span],
                    hop_send.at[step, p, landed],
                    hop_recv.at[step, p, landed],
                    neighbours[order[step] - 1],
                )
                copy.start()
                started.append((landed, span, copy))
        for landed, span, copy in started:
            copy.wait_recv()
            held[landed, :, span] += hop_in[step, landed, :, span].astype(jnp.float32)
            hops.append(copy)
    out_ref[...] = (stream_ref[...].astype(jnp.float32) + held[0]).astype(jnp.bfloat16)
    for copy in copies + core_copies + hops:
        copy.wait_send()


def output(stream, gated, scaling, out_weight, heads, groups):
    rows, cols = stream.shape
    batch = rows * heads
    group_rows, size = gated.shape
    dims = heads.bit_length() - 2
    chips = 1 << dims
    parts = len(parts_of(cols, dims))
    extra = groups - 1
    dma = pltpu.SemaphoreType.DMA
    flat = jnp.broadcast_to(scaling.astype(jnp.bfloat16)[None, :], (SMALL, group_rows))
    return pl.pallas_call(
        functools.partial(output_kernel, heads, groups),
        in_specs=[VMEM] * 4,
        out_specs=VMEM,
        out_shape=jax.ShapeDtypeStruct(stream.shape, stream.dtype),
        scratch_shapes=[
            pltpu.VMEM((batch, size), jnp.bfloat16),
            pltpu.VMEM((groups, SMALL, group_rows), jnp.bfloat16),
            pltpu.VMEM((batch, 128), jnp.float32),
            pltpu.VMEM((chips, rows, cols), jnp.float32),
            pltpu.VMEM((chips, rows, cols), jnp.bfloat16),
            pltpu.VMEM((chips, rows, cols), jnp.bfloat16),
            pltpu.VMEM((dims, chips, rows, cols), jnp.bfloat16),
            pltpu.VMEM((dims, chips, rows, cols), jnp.bfloat16),
            dma((extra,)),
            dma((extra,)),
            dma((extra,)),
            dma((extra,)),
            dma((chips,)),
            dma((chips,)),
            dma((dims, parts, chips)),
            dma((dims, parts, chips)),
        ],
        compiler_params=pltpu.CompilerParams(
            collective_id=1, has_side_effects=True, vmem_limit_bytes=48 * 1024 * 1024
        ),
    )(stream, gated, flat, out_weight)


def per_device(
    stream,
    norm_gain,
    query_weight,
    key_weight,
    value_weight,
    gate_weight,
    write_weight,
    decay_weight,
    decay_rate,
    head_gain,
    out_weight,
    state,
):
    heads = decay_rate.shape[0]
    groups = lax.axis_size("tp") // heads
    weights = (query_weight, key_weight, value_weight, gate_weight)
    packed = project(
        stream, norm_gain, weights, write_weight, decay_weight, decay_rate, heads, groups
    )
    size = head_gain.shape[0]
    updated, readout = state_step(state, packed)
    gate = packed[:, 6 * size :]
    scaling = lax.rsqrt(jnp.mean(readout * readout, axis=1) + EPS)
    gated = (readout * head_gain.astype(jnp.float32)[None, :] * jax.nn.silu(gate)).astype(
        jnp.bfloat16
    )
    result = output(stream, gated, scaling, out_weight, heads, groups)
    return (result, updated)


def solution(mesh):
    placed = (
        P("tp", None),
        P(),
        P("tp", None),
        P("tp", None),
        P("tp", None),
        P("tp", None),
        P(),
        P(),
        P(),
        P(),
        P("tp", None),
        P("tp", None, None),
    )
    return jax.shard_map(
        per_device,
        mesh=mesh,
        in_specs=placed,
        out_specs=(P("tp", None), P("tp", None, None)),
        check_vma=False,
    )
```

```python
import functools

import jax
import jax.numpy as jnp
from jax import lax
from jax.experimental import pallas as pl
from jax.experimental.pallas import tpu as pltpu
from jax.sharding import PartitionSpec as P

EPS = 1e-06
MESH = pl.DeviceIdType.MESH
VMEM = pl.BlockSpec(memory_space=pltpu.VMEM)
SMALL = 16


def flip(me, bits):
    other = me
    for bit in bits:
        other = other + (1 - 2 * ((me // (1 << bit)) % 2)) * (1 << bit)
    return other


def parts_of(cols, dims):
    tiles = cols // 128
    count = max(1, min(dims, tiles))
    cuts = [tiles * i // count * 128 for i in range(count + 1)]
    ranges = [(cuts[i], cuts[i + 1] - cuts[i]) for i in range(count)]
    orders = [[1 + (i + j) % dims for j in range(dims)] for i in range(count)]
    return list(zip(ranges, orders))


def masks_of(order):
    sets = [((), -1)]
    for step in range(len(order)):
        sets = sets + [(bits + (order[step],), step) for bits, _ in sets]
    return sets


def key_of(bits):
    return sum(1 << (bit - 1) for bit in bits)


def enter(devices):
    barrier = pltpu.get_barrier_semaphore()
    for device in devices:
        pl.semaphore_signal(barrier, inc=1, device_id=(device,), device_id_type=MESH)
    pl.semaphore_wait(barrier, len(devices))


def remote(source, target, send_sem, recv_sem, device):
    return pltpu.make_async_remote_copy(
        src_ref=source,
        dst_ref=target,
        send_sem=send_sem,
        recv_sem=recv_sem,
        device_id=(device,),
        device_id_type=MESH,
    )


def project_kernel(
    heads,
    groups,
    stream_ref,
    gain_ref,
    query_w,
    key_w,
    value_w,
    gate_w,
    write_w,
    decay_w,
    rate_ref,
    packed_out,
    gathered,
    weights,
    write_t,
    decay_t,
    local_sems,
    partial,
    sent,
    received,
    small_sent,
    small_received,
    turned,
    ici_send,
    ici_recv,
    core_send,
    core_recv,
    group_send,
    group_recv,
    small_send,
    small_recv,
):
    me = lax.axis_index("tp")
    place = me % heads
    group = me // heads
    rows, cols = stream_ref.shape
    batch = gathered.shape[0]
    group_rows = batch // groups
    dims = heads.bit_length() - 2
    sibling = flip(me, (0,))
    neighbours = [flip(me, (bit,)) for bit in range(1, dims + 1)]
    others = [place + heads * ((group + j) % groups) for j in range(1, groups)]
    size = query_w.shape[1]
    own_cols = pl.ds(pl.multiple_of(group * cols, cols), cols)
    fetches = [
        pltpu.make_async_copy(
            weight, weights.at[:, i * size : (i + 1) * size], local_sems.at[i]
        )
        for i, weight in enumerate((query_w, key_w, value_w, gate_w))
    ] + [
        pltpu.make_async_copy(source.at[:, own_cols], target, local_sems.at[4 + i])
        for i, (source, target) in enumerate(((write_w, write_t), (decay_w, decay_t)))
    ]
    for fetch in fetches:
        fetch.start()
    enter([sibling] + neighbours + others)

    halves = 2 if rows % 32 == 0 and group_rows % rows == 0 else 1
    part_rows = rows // halves
    half_batch = batch // halves
    ranges = parts_of(cols, dims)

    def half_rows(h, device_place):
        begin = h * half_batch + device_place * part_rows
        return pl.ds(pl.multiple_of(begin, part_rows), part_rows)

    def block(h, device_place, part):
        return gathered.at[half_rows(h, device_place), pl.ds(part[0][0], part[0][1])]

    sends = []
    core_copies = [[] for _ in range(halves)]

    def pass_on(h, p, part, bits, step):
        order = part[1]
        origin = flip(place, bits)
        target = block(h, origin, part)
        if bits:
            source = target
        else:
            source = stream_ref.at[
                pl.ds(h * part_rows, part_rows), pl.ds(part[0][0], part[0][1])
            ]
        for later in range(step + 1, dims):
            landed = key_of(bits + (order[later],))
            copy = remote(
                source,
                target,
                ici_send.at[h, p, landed],
                ici_recv.at[h, p, landed],
                flip(me, (order[later],)),
            )
            copy.start()
            sends.append(copy)
        own = key_of(bits)
        copy = remote(source, target, core_send.at[h, p, own], core_recv.at[h, p, own], sibling)
        copy.start()
        core_copies[h].append(copy)

    def begin(h):
        for p, part in enumerate(ranges):
            pass_on(h, p, part, (), -1)

    def relay(h, index):
        for p, part in enumerate(ranges):
            bits, step = masks_of(part[1])[index]
            landed = key_of(bits)
            target = block(h, flip(place, bits), part)
            remote(
                target, target, ici_send.at[h, p, landed], ici_recv.at[h, p, landed], sibling
            ).wait_recv()
            pass_on(h, p, part, bits, step)

    early = max(2, 1 << (dims - 1))
    begin(0)
    for h in range(halves):
        gathered[half_rows(h, place), :] = stream_ref[h * part_rows : (h + 1) * part_rows, :]
    relay(0, 1)
    for h in range(1, halves):
        begin(h)
    for index in range(2, 1 << dims):
        relay(0, index)
    for h in range(1, halves):
        for index in range(1, early):
            relay(h, index)
    for copy in core_copies[0]:
        copy.wait_recv()

    gain = gain_ref[group].astype(jnp.float32)
    for fetch in fetches:
        fetch.wait()

    def project(begin, count, at):
        x = gathered[pl.ds(begin, count), :].astype(jnp.float32)
        gained = (x * gain).astype(jnp.bfloat16)
        partial[pl.ds(at, count), :] = jnp.dot(
            gained, weights[...], preferred_element_type=jnp.float32
        )
        mine = lax.broadcasted_iota(jnp.int32, (count, heads), 1) == place
        pre = [
            jnp.sum(
                jnp.where(
                    mine,
                    lax.dot_general(
                        gained,
                        w[...],
                        (((1,), (1,)), ((), ())),
                        preferred_element_type=jnp.float32,
                    ),
                    0.0,
                ),
                axis=1,
                keepdims=True,
            )
            for w in (write_t, decay_t)
        ]
        squares = jnp.sum(x * x, axis=1, keepdims=True)
        lane = lax.broadcasted_iota(jnp.int32, (count, 128), 1)
        return jnp.where(
            lane == 0, pre[0], jnp.where(lane == 1, pre[1], jnp.where(lane == 2, squares, 0.0))
        )

    copies = []
    wide = max(group_rows, 128)
    count = group_rows // halves

    def half_of(h, target_group):
        begin = h * half_batch + target_group * count
        return pl.multiple_of(begin, count)

    for h in range(halves):
        if h:
            for index in range(early, 1 << dims):
                relay(h, index)
            for copy in core_copies[h]:
                copy.wait_recv()
        for j in range(1, groups):
            spot = slice(h * count, (h + 1) * count)
            side = project(half_of(h, (group + j) % groups), count, 0)
            sent[j - 1, spot] = partial[0:count].astype(jnp.bfloat16)
            turned[spot] = side
            routes = [(sent.at[j - 1, spot], received.at[j - 1, spot], group_send, group_recv)]
            flat = turned[...].T
            small_sent[j - 1, :, spot] = flat[0:SMALL, spot].astype(jnp.bfloat16)
            routes.append(
                (
                    small_sent.at[j - 1, :, spot],
                    small_received.at[j - 1, :, spot],
                    small_send,
                    small_recv,
                )
            )
            for source, target, send, recv in routes:
                copy = remote(
                    source, target, send.at[h, j - 1], recv.at[h, j - 1], others[j - 1]
                )
                copy.start()
                copies.append(copy)
    for h in range(halves):
        turned[h * count : (h + 1) * count] = project(half_of(h, group), count, h * count)
    total = partial[...]
    flat = turned[...].T[0:SMALL, :]
    for copy in copies:
        copy.wait_recv()
    for j in range(1, groups):
        total = total + received[j - 1].astype(jnp.float32)
    small_total = flat[:, 0:group_rows]
    for j in range(1, groups):
        small_total = small_total + small_received[j - 1].astype(jnp.float32)
    turned_back = jnp.concatenate(
        [small_total, jnp.zeros((SMALL, wide - group_rows), jnp.float32)], axis=1
    ) if wide > group_rows else small_total
    side = jnp.concatenate(
        [turned_back, jnp.zeros((128 - SMALL, wide), jnp.float32)], axis=0
    ).T[0:group_rows]
    scale = lax.rsqrt(side[:, 2:3] / (cols * groups) + EPS)

    def rounded(v):
        return v.astype(jnp.bfloat16).astype(jnp.float32)

    projected = rounded(total * scale)
    query = projected[:, :size]
    key = projected[:, size : 2 * size]
    query = query * lax.rsqrt(jnp.sum(query * query, axis=1, keepdims=True) + EPS) * size**-0.5
    key = key * lax.rsqrt(jnp.sum(key * key, axis=1, keepdims=True) + EPS)
    pre = rounded(side * scale)
    strength = jax.nn.sigmoid(pre[:, 0:1])
    mine = lax.broadcasted_iota(jnp.int32, rate_ref.shape, 1) == place
    rate = jnp.sum(jnp.where(mine, rate_ref[...], 0.0), axis=1, keepdims=True)
    decay = pre[:, 1:2]
    softplus = jnp.maximum(decay, 0.0) + jnp.log(1.0 + jnp.exp(-jnp.abs(decay)))
    factor = jnp.exp(-rate * softplus)
    overlap = jnp.sum(query * key, axis=1, keepdims=True)
    results = [jnp.broadcast_to(v, (group_rows, size)) for v in (strength, factor, overlap)]
    results += [query, key, projected[:, 2 * size :]]
    for i, v in enumerate(results):
        span = pl.ds(i * size, v.shape[1])
        if halves == 1:
            packed_out[:, span] = v
            continue
        for h in range(halves):
            for q in range(group_rows // rows):
                to, come = q * rows + h * part_rows, h * count + q * part_rows
                packed_out[to : to + part_rows, span] = v[come : come + part_rows]
    for copy in sends + sum(core_copies, []) + copies:
        copy.wait_send()


def project(stream, norm_gain, weights, write_weight, decay_weight, rate, heads, groups):
    rows, cols = stream.shape
    batch = rows * heads
    group_rows = batch // groups
    size = weights[0].shape[1]
    dims = heads.bit_length() - 2
    parts = len(parts_of(cols, dims))
    extra = groups - 1
    halves = 2
    dma = pltpu.SemaphoreType.DMA
    anywhere = pl.BlockSpec(memory_space=pl.ANY)
    return pl.pallas_call(
        functools.partial(project_kernel, heads, groups),
        in_specs=[VMEM] * 2 + [anywhere] * 6 + [VMEM],
        out_specs=VMEM,
        out_shape=jax.ShapeDtypeStruct((group_rows, 7 * size), jnp.float32),
        scratch_shapes=[
            pltpu.VMEM((batch, cols), jnp.bfloat16),
            pltpu.VMEM((cols, 4 * size), jnp.bfloat16),
            pltpu.VMEM((heads, cols), jnp.bfloat16),
            pltpu.VMEM((heads, cols), jnp.bfloat16),
            dma((6,)),
            pltpu.VMEM((group_rows, 4 * size), jnp.float32),
            pltpu.VMEM((extra, group_rows, 4 * size), jnp.bfloat16),
            pltpu.VMEM((extra, group_rows, 4 * size), jnp.bfloat16),
            pltpu.VMEM((extra, SMALL, group_rows), jnp.bfloat16),
            pltpu.VMEM((extra, SMALL, group_rows), jnp.bfloat16),
            pltpu.VMEM((max(group_rows, 128), 128), jnp.float32),
            dma((halves, parts, 1 << dims)),
            dma((halves, parts, 1 << dims)),
            dma((halves, parts, 1 << dims)),
            dma((halves, parts, 1 << dims)),
            dma((halves, extra)),
            dma((halves, extra)),
            dma((halves, extra)),
            dma((halves, extra)),
        ],
        compiler_params=pltpu.CompilerParams(
            collective_id=0, has_side_effects=True
        ),
    )(
        stream,
        norm_gain.reshape(groups, 1, cols),
        *weights,
        write_weight.T,
        decay_weight.T,
        rate.reshape(1, heads),
    )


def split(v):
    high = v.astype(jnp.bfloat16)
    return high, (v - high.astype(jnp.float32)).astype(jnp.bfloat16)


def state_kernel(
    state_ref, packed_ref, gain_ref, new_ref, gated_ref, flat_ref, held, readout, in_sems, out_sems
):
    total, size, _ = state_ref.shape
    steps = in_sems.shape[0]
    count = total // steps

    def rows_of(step):
        return pl.ds(pl.multiple_of(step * count, count), count)

    def fetch(step):
        rows = rows_of(step)
        return pltpu.make_async_copy(state_ref.at[rows], held.at[rows], in_sems.at[step])

    def store(step):
        rows = rows_of(step)
        return pltpu.make_async_copy(held.at[rows], new_ref.at[rows], out_sems.at[step])

    for step in range(steps):
        fetch(step).start()
    spots = lax.broadcasted_iota(jnp.int32, (4 * count, size), 0) % count

    def diagonal(rows):
        marks = spots[0 : rows.shape[0]]
        return jnp.concatenate(
            [jnp.where(marks == b, rows, jnp.zeros_like(rows)) for b in range(count)], axis=1
        )

    def body(step, carry):
        rows = rows_of(step)

        def columns(first, width=1):
            return packed_ref[rows, first * size : (first + width) * size]

        key_high, key_low = split(columns(4))
        query_high, query_low = split(columns(3))
        four = jnp.concatenate([key_high, key_low, query_high, query_low], axis=0)
        strength, factor, overlap = columns(0), columns(1), columns(2)
        left = jnp.concatenate([key_high, key_low, key_high], axis=0)
        left = jnp.concatenate([left, jnp.zeros((size - 3 * count, size), left.dtype)], axis=0)
        left = left.astype(jnp.float32).T.astype(jnp.bfloat16)[:, 0 : 3 * count]
        wide = diagonal(four)
        fetch(step).wait()
        memory = held[rows].reshape(count * size, size).astype(jnp.bfloat16)
        both = jnp.dot(wide, memory, preferred_element_type=jnp.float32)
        recalled = both[0:count] + both[count : 2 * count]
        asked = both[2 * count : 3 * count] + both[3 * count : 4 * count]
        change = strength * (columns(5) - factor * recalled)
        readout[rows, :] = factor * asked + overlap * change
        change_high, change_low = split(change)
        right = diagonal(jnp.concatenate([change_high, change_high, change_low], axis=0))
        outer = jnp.dot(left, right, preferred_element_type=jnp.float32)
        for b in range(count):
            spot = step * count + b
            held[spot] = factor[b : b + 1, :] * held[spot] + outer[:, b * size : (b + 1) * size]
        store(step).start()
        return carry

    lax.fori_loop(0, steps, body, 0)
    read = readout[...]
    scaling = lax.rsqrt(jnp.sum(read * read, axis=1, keepdims=True) / size + EPS)
    gate = packed_ref[:, 6 * size :]
    gated_ref[...] = (
        read * gain_ref[...].astype(jnp.float32) * (gate / (1.0 + jnp.exp(-gate)))
    ).astype(jnp.bfloat16)
    tall = jnp.broadcast_to(scaling, (total, 128))
    if total < 128:
        tall = jnp.concatenate([tall, jnp.zeros((128 - total, 128), jnp.float32)], axis=0)
    flat_ref[...] = tall.T[0:SMALL, 0:total].astype(jnp.bfloat16)
    for step in range(steps):
        store(step).wait()


def state_step(state, packed, head_gain):
    count, size, _ = state.shape
    steps = count // min(16, count)
    anywhere = pl.BlockSpec(memory_space=pl.ANY)
    return pl.pallas_call(
        state_kernel,
        in_specs=[anywhere, VMEM, VMEM],
        out_specs=[anywhere, VMEM, VMEM],
        out_shape=[
            jax.ShapeDtypeStruct(state.shape, state.dtype),
            jax.ShapeDtypeStruct((count, size), jnp.bfloat16),
            jax.ShapeDtypeStruct((SMALL, count), jnp.bfloat16),
        ],
        scratch_shapes=[
            pltpu.VMEM(state.shape, state.dtype),
            pltpu.VMEM((count, size), jnp.float32),
            pltpu.SemaphoreType.DMA((steps,)),
            pltpu.SemaphoreType.DMA((steps,)),
        ],
    )(state, packed, head_gain.reshape(1, size))


def output_kernel(
    heads,
    groups,
    stream_ref,
    gated_ref,
    scaling_ref,
    weight_hbm,
    out_ref,
    weight_ref,
    weight_sem,
    all_gated,
    all_scaling,
    columns,
    held,
    core_out,
    core_in,
    hop_out,
    hop_in,
    gated_send,
    gated_recv,
    scaling_send,
    scaling_recv,
    core_send,
    core_recv,
    hop_send,
    hop_recv,
):
    me = lax.axis_index("tp")
    place = me % heads
    group = me // heads
    rows, cols = stream_ref.shape
    batch = all_gated.shape[0]
    group_rows = batch // groups
    dims = heads.bit_length() - 2
    chips = 1 << dims
    sibling = flip(me, (0,))
    neighbours = [flip(me, (bit,)) for bit in range(1, dims + 1)]
    others = [place + heads * ((group + j) % groups) for j in range(1, groups)]
    weight_copy = pltpu.make_async_copy(weight_hbm, weight_ref, weight_sem)
    weight_copy.start()
    enter([sibling] + neighbours + others)
    own_rows = pl.ds(pl.multiple_of(group * group_rows, group_rows), group_rows)
    copies = []
    arriving = []
    for j in range(1, groups):
        for source, target, send, recv in (
            (gated_ref, all_gated.at[own_rows], gated_send, gated_recv),
            (scaling_ref, all_scaling.at[group], scaling_send, scaling_recv),
        ):
            copy = remote(source, target, send.at[j - 1], recv.at[j - 1], others[j - 1])
            copy.start()
            copies.append(copy)
    all_gated[own_rows, :] = gated_ref[...]
    all_scaling[group] = scaling_ref[...]
    for copy in copies:
        copy.wait_recv()
    weight_copy.wait()
    wide = max(group_rows, 128)
    for g in range(groups):
        flat = all_scaling[g].astype(jnp.float32)
        if wide > group_rows:
            flat = jnp.concatenate(
                [flat, jnp.zeros((SMALL, wide - group_rows), jnp.float32)], axis=1
            )
        flat = jnp.concatenate([flat, jnp.zeros((128 - SMALL, wide), jnp.float32)], axis=0)
        columns[g * group_rows : (g + 1) * group_rows, :] = flat.T[0:group_rows]

    def relative(owner, mask):
        bits = tuple(bit for bit in range(1, dims + 1) if mask >> (bit - 1) & 1)
        begin = flip(owner, bits) * rows
        return pl.ds(pl.multiple_of(begin, rows), rows)

    def head_rows(owner, masks):
        picks = [relative(owner, mask) for mask in masks]
        left = jnp.concatenate([all_gated[pick, :] for pick in picks], axis=0)
        scale = jnp.concatenate([columns[pick, 0:1] for pick in picks], axis=0)
        product = lax.dot_general(
            left, weight_ref[...], (((1,), (1,)), ((), ())), preferred_element_type=jnp.float32
        )
        return product * scale

    core_copies = [
        remote(
            core_out.at[mask], core_in.at[mask], core_send.at[mask], core_recv.at[mask], sibling
        )
        for mask in range(chips)
    ]
    batch_of = min(4, chips)
    sweep = list(range(chips - 1, -1, -1))
    for first in range(0, chips, batch_of):
        masks = sweep[first : first + batch_of]
        product = head_rows(flip(place, (0,)), masks).astype(jnp.bfloat16)
        for i, mask in enumerate(masks):
            core_out[mask] = product[i * rows : (i + 1) * rows]
            core_copies[mask].start()
    for first in range(0, chips, batch_of):
        masks = sweep[first : first + batch_of]
        product = head_rows(place, masks)
        for i, mask in enumerate(masks):
            held[mask] = product[i * rows : (i + 1) * rows]
    for mask in sweep:
        core_copies[mask].wait_recv()
        held[mask] += core_in[mask].astype(jnp.float32)

    parts = parts_of(cols, dims)
    hops = []
    for step in range(dims):
        started = []
        for p, ((start, width), order) in enumerate(parts):
            span = pl.ds(start, width)
            crossed = [1 << (bit - 1) for bit in order[:step]]
            now = 1 << (order[step] - 1)
            for mask in range(chips):
                if any(mask & c for c in crossed) or not mask & now:
                    continue
                landed = mask - now
                hop_out[step, landed, :, span] = held[mask, :, span].astype(jnp.bfloat16)
                copy = remote(
                    hop_out.at[step, landed, :, span],
                    hop_in.at[step, landed, :, span],
                    hop_send.at[step, p, landed],
                    hop_recv.at[step, p, landed],
                    neighbours[order[step] - 1],
                )
                copy.start()
                started.append((landed, span, copy))
        for landed, span, copy in started:
            copy.wait_recv()
            held[landed, :, span] += hop_in[step, landed, :, span].astype(jnp.float32)
            hops.append(copy)
    out_ref[...] = (stream_ref[...].astype(jnp.float32) + held[0]).astype(jnp.bfloat16)
    for copy in copies + core_copies + hops:
        copy.wait_send()


def output(stream, gated, scaling, out_weight, heads, groups):
    rows, cols = stream.shape
    batch = rows * heads
    group_rows, size = gated.shape
    dims = heads.bit_length() - 2
    chips = 1 << dims
    parts = len(parts_of(cols, dims))
    extra = groups - 1
    dma = pltpu.SemaphoreType.DMA
    anywhere = pl.BlockSpec(memory_space=pl.ANY)
    return pl.pallas_call(
        functools.partial(output_kernel, heads, groups),
        in_specs=[VMEM] * 3 + [anywhere],
        out_specs=VMEM,
        out_shape=jax.ShapeDtypeStruct(stream.shape, stream.dtype),
        scratch_shapes=[
            pltpu.VMEM(out_weight.shape, out_weight.dtype),
            dma(()),
            pltpu.VMEM((batch, size), jnp.bfloat16),
            pltpu.VMEM((groups, SMALL, group_rows), jnp.bfloat16),
            pltpu.VMEM((batch, 128), jnp.float32),
            pltpu.VMEM((chips, rows, cols), jnp.float32),
            pltpu.VMEM((chips, rows, cols), jnp.bfloat16),
            pltpu.VMEM((chips, rows, cols), jnp.bfloat16),
            pltpu.VMEM((dims, chips, rows, cols), jnp.bfloat16),
            pltpu.VMEM((dims, chips, rows, cols), jnp.bfloat16),
            dma((extra,)),
            dma((extra,)),
            dma((extra,)),
            dma((extra,)),
            dma((chips,)),
            dma((chips,)),
            dma((dims, parts, chips)),
            dma((dims, parts, chips)),
        ],
        compiler_params=pltpu.CompilerParams(
            collective_id=1, has_side_effects=True
        ),
    )(stream, gated, scaling, out_weight)


def per_device(
    stream,
    norm_gain,
    query_weight,
    key_weight,
    value_weight,
    gate_weight,
    write_weight,
    decay_weight,
    decay_rate,
    head_gain,
    out_weight,
    state,
):
    heads = decay_rate.shape[0]
    groups = lax.axis_size("tp") // heads
    weights = (query_weight, key_weight, value_weight, gate_weight)
    packed = project(
        stream, norm_gain, weights, write_weight, decay_weight, decay_rate, heads, groups
    )
    updated, gated, scaling = state_step(state, packed, head_gain)
    result = output(stream, gated, scaling, out_weight, heads, groups)
    return (result, updated)


def solution(mesh):
    placed = (
        P("tp", None),
        P(),
        P("tp", None),
        P("tp", None),
        P("tp", None),
        P("tp", None),
        P(),
        P(),
        P(),
        P(),
        P("tp", None),
        P("tp", None, None),
    )
    return jax.shard_map(
        per_device,
        mesh=mesh,
        in_specs=placed,
        out_specs=(P("tp", None), P("tp", None, None)),
        check_vma=False,
    )
```

```python
import functools

import jax
import jax.numpy as jnp
from jax import lax
from jax.experimental import pallas as pl
from jax.experimental.pallas import tpu as pltpu
from jax.sharding import PartitionSpec as P

EPS = 1e-06
MESH = pl.DeviceIdType.MESH
VMEM = pl.BlockSpec(memory_space=pltpu.VMEM)
SMALL = 16


def flip(me, bits):
    other = me
    for bit in bits:
        other = other + (1 - 2 * ((me // (1 << bit)) % 2)) * (1 << bit)
    return other


def parts_of(cols, dims):
    tiles = cols // 128
    count = max(1, min(dims, tiles))
    cuts = [tiles * i // count * 128 for i in range(count + 1)]
    ranges = [(cuts[i], cuts[i + 1] - cuts[i]) for i in range(count)]
    orders = [[1 + (i + j) % dims for j in range(dims)] for i in range(count)]
    return list(zip(ranges, orders))


def masks_of(order):
    sets = [((), -1)]
    for step in range(len(order)):
        sets = sets + [(bits + (order[step],), step) for bits, _ in sets]
    return sets


def key_of(bits):
    return sum(1 << (bit - 1) for bit in bits)


def enter(devices):
    barrier = pltpu.get_barrier_semaphore()
    for device in devices:
        pl.semaphore_signal(barrier, inc=1, device_id=(device,), device_id_type=MESH)
    pl.semaphore_wait(barrier, len(devices))


def remote(source, target, send_sem, recv_sem, device):
    return pltpu.make_async_remote_copy(
        src_ref=source,
        dst_ref=target,
        send_sem=send_sem,
        recv_sem=recv_sem,
        device_id=(device,),
        device_id_type=MESH,
    )


def project_kernel(
    heads,
    groups,
    stream_ref,
    gain_ref,
    query_w,
    key_w,
    value_w,
    gate_w,
    write_w,
    decay_w,
    rate_ref,
    packed_out,
    gathered,
    weights,
    write_t,
    decay_t,
    local_sems,
    partial,
    sent,
    received,
    small_sent,
    small_received,
    turned,
    ici_send,
    ici_recv,
    core_send,
    core_recv,
    group_send,
    group_recv,
    small_send,
    small_recv,
):
    me = lax.axis_index("tp")
    place = me % heads
    group = me // heads
    rows, cols = stream_ref.shape
    batch = gathered.shape[0]
    group_rows = batch // groups
    dims = heads.bit_length() - 2
    sibling = flip(me, (0,))
    neighbours = [flip(me, (bit,)) for bit in range(1, dims + 1)]
    others = [place + heads * ((group + j) % groups) for j in range(1, groups)]
    size = query_w.shape[1]
    own_cols = pl.ds(pl.multiple_of(group * cols, cols), cols)
    fetches = [
        pltpu.make_async_copy(
            weight, weights.at[:, i * size : (i + 1) * size], local_sems.at[i]
        )
        for i, weight in enumerate((query_w, key_w, value_w, gate_w))
    ] + [
        pltpu.make_async_copy(source.at[:, own_cols], target, local_sems.at[4 + i])
        for i, (source, target) in enumerate(((write_w, write_t), (decay_w, decay_t)))
    ]
    for fetch in fetches:
        fetch.start()
    enter([sibling] + neighbours + others)

    halves = 2 if rows % 32 == 0 and group_rows % rows == 0 else 1
    part_rows = rows // halves
    half_batch = batch // halves
    ranges = parts_of(cols, dims)

    def half_rows(h, device_place):
        begin = h * half_batch + device_place * part_rows
        return pl.ds(pl.multiple_of(begin, part_rows), part_rows)

    def block(h, device_place, part):
        return gathered.at[half_rows(h, device_place), pl.ds(part[0][0], part[0][1])]

    sends = []
    core_copies = [[] for _ in range(halves)]

    def pass_on(h, p, part, bits, step):
        order = part[1]
        origin = flip(place, bits)
        target = block(h, origin, part)
        if bits:
            source = target
        else:
            source = stream_ref.at[
                pl.ds(h * part_rows, part_rows), pl.ds(part[0][0], part[0][1])
            ]
        for later in range(step + 1, dims):
            landed = key_of(bits + (order[later],))
            copy = remote(
                source,
                target,
                ici_send.at[h, p, landed],
                ici_recv.at[h, p, landed],
                flip(me, (order[later],)),
            )
            copy.start()
            sends.append(copy)
        own = key_of(bits)
        copy = remote(source, target, core_send.at[h, p, own], core_recv.at[h, p, own], sibling)
        copy.start()
        core_copies[h].append(copy)

    def begin(h):
        for p, part in enumerate(ranges):
            pass_on(h, p, part, (), -1)

    def relay(h, index):
        for p, part in enumerate(ranges):
            bits, step = masks_of(part[1])[index]
            landed = key_of(bits)
            target = block(h, flip(place, bits), part)
            remote(
                target, target, ici_send.at[h, p, landed], ici_recv.at[h, p, landed], sibling
            ).wait_recv()
            pass_on(h, p, part, bits, step)

    early = max(2, 1 << (dims - 1))
    begin(0)
    for h in range(halves):
        gathered[half_rows(h, place), :] = stream_ref[h * part_rows : (h + 1) * part_rows, :]
    relay(0, 1)
    for h in range(1, halves):
        begin(h)
    for index in range(2, 1 << dims):
        relay(0, index)
    for h in range(1, halves):
        for index in range(1, early):
            relay(h, index)
    for copy in core_copies[0]:
        copy.wait_recv()

    gain = gain_ref[group].astype(jnp.float32)
    for fetch in fetches:
        fetch.wait()

    def project(begin, count, at):
        x = gathered[pl.ds(begin, count), :].astype(jnp.float32)
        gained = (x * gain).astype(jnp.bfloat16)
        partial[pl.ds(at, count), :] = jnp.dot(
            gained, weights[...], preferred_element_type=jnp.float32
        )
        mine = lax.broadcasted_iota(jnp.int32, (count, heads), 1) == place
        pre = [
            jnp.sum(
                jnp.where(
                    mine,
                    lax.dot_general(
                        gained,
                        w[...],
                        (((1,), (1,)), ((), ())),
                        preferred_element_type=jnp.float32,
                    ),
                    0.0,
                ),
                axis=1,
                keepdims=True,
            )
            for w in (write_t, decay_t)
        ]
        squares = jnp.sum(x * x, axis=1, keepdims=True)
        lane = lax.broadcasted_iota(jnp.int32, (count, 128), 1)
        return jnp.where(
            lane == 0, pre[0], jnp.where(lane == 1, pre[1], jnp.where(lane == 2, squares, 0.0))
        )

    copies = []
    wide = max(group_rows, 128)
    count = group_rows // halves

    def half_of(h, target_group):
        begin = h * half_batch + target_group * count
        return pl.multiple_of(begin, count)

    for h in range(halves):
        if h:
            for index in range(early, 1 << dims):
                relay(h, index)
            for copy in core_copies[h]:
                copy.wait_recv()
        for j in range(1, groups):
            spot = slice(h * count, (h + 1) * count)
            side = project(half_of(h, (group + j) % groups), count, 0)
            sent[j - 1, spot] = partial[0:count].astype(jnp.bfloat16)
            turned[spot] = side
            routes = [(sent.at[j - 1, spot], received.at[j - 1, spot], group_send, group_recv)]
            flat = turned[...].T
            small_sent[j - 1, :, spot] = flat[0:SMALL, spot].astype(jnp.bfloat16)
            routes.append(
                (
                    small_sent.at[j - 1, :, spot],
                    small_received.at[j - 1, :, spot],
                    small_send,
                    small_recv,
                )
            )
            for source, target, send, recv in routes:
                copy = remote(
                    source, target, send.at[h, j - 1], recv.at[h, j - 1], others[j - 1]
                )
                copy.start()
                copies.append(copy)
    for h in range(halves):
        turned[h * count : (h + 1) * count] = project(half_of(h, group), count, h * count)
    total = partial[...]
    flat = turned[...].T[0:SMALL, :]
    for copy in copies:
        copy.wait_recv()
    for j in range(1, groups):
        total = total + received[j - 1].astype(jnp.float32)
    small_total = flat[:, 0:group_rows]
    for j in range(1, groups):
        small_total = small_total + small_received[j - 1].astype(jnp.float32)
    turned_back = jnp.concatenate(
        [small_total, jnp.zeros((SMALL, wide - group_rows), jnp.float32)], axis=1
    ) if wide > group_rows else small_total
    side = jnp.concatenate(
        [turned_back, jnp.zeros((128 - SMALL, wide), jnp.float32)], axis=0
    ).T[0:group_rows]
    scale = lax.rsqrt(side[:, 2:3] / (cols * groups) + EPS)

    def rounded(v):
        return v.astype(jnp.bfloat16).astype(jnp.float32)

    projected = rounded(total * scale)
    query = projected[:, :size]
    key = projected[:, size : 2 * size]
    query = query * lax.rsqrt(jnp.sum(query * query, axis=1, keepdims=True) + EPS) * size**-0.5
    key = key * lax.rsqrt(jnp.sum(key * key, axis=1, keepdims=True) + EPS)
    pre = rounded(side * scale)
    strength = jax.nn.sigmoid(pre[:, 0:1])
    mine = lax.broadcasted_iota(jnp.int32, rate_ref.shape, 1) == place
    rate = jnp.sum(jnp.where(mine, rate_ref[...], 0.0), axis=1, keepdims=True)
    decay = pre[:, 1:2]
    softplus = jnp.maximum(decay, 0.0) + jnp.log(1.0 + jnp.exp(-jnp.abs(decay)))
    factor = jnp.exp(-rate * softplus)
    overlap = jnp.sum(query * key, axis=1, keepdims=True)
    results = [jnp.broadcast_to(v, (group_rows, size)) for v in (strength, factor, overlap)]
    results += [query, key, projected[:, 2 * size :]]
    for i, v in enumerate(results):
        span = pl.ds(i * size, v.shape[1])
        if halves == 1:
            packed_out[:, span] = v
            continue
        for h in range(halves):
            for q in range(group_rows // rows):
                to, come = q * rows + h * part_rows, h * count + q * part_rows
                packed_out[to : to + part_rows, span] = v[come : come + part_rows]
    for copy in sends + sum(core_copies, []) + copies:
        copy.wait_send()


def project(stream, norm_gain, weights, write_weight, decay_weight, rate, heads, groups):
    rows, cols = stream.shape
    batch = rows * heads
    group_rows = batch // groups
    size = weights[0].shape[1]
    dims = heads.bit_length() - 2
    parts = len(parts_of(cols, dims))
    extra = groups - 1
    halves = 2
    dma = pltpu.SemaphoreType.DMA
    anywhere = pl.BlockSpec(memory_space=pl.ANY)
    return pl.pallas_call(
        functools.partial(project_kernel, heads, groups),
        in_specs=[VMEM] * 2 + [anywhere] * 6 + [VMEM],
        out_specs=VMEM,
        out_shape=jax.ShapeDtypeStruct((group_rows, 7 * size), jnp.float32),
        scratch_shapes=[
            pltpu.VMEM((batch, cols), jnp.bfloat16),
            pltpu.VMEM((cols, 4 * size), jnp.bfloat16),
            pltpu.VMEM((heads, cols), jnp.bfloat16),
            pltpu.VMEM((heads, cols), jnp.bfloat16),
            dma((6,)),
            pltpu.VMEM((group_rows, 4 * size), jnp.float32),
            pltpu.VMEM((extra, group_rows, 4 * size), jnp.bfloat16),
            pltpu.VMEM((extra, group_rows, 4 * size), jnp.bfloat16),
            pltpu.VMEM((extra, SMALL, group_rows), jnp.bfloat16),
            pltpu.VMEM((extra, SMALL, group_rows), jnp.bfloat16),
            pltpu.VMEM((max(group_rows, 128), 128), jnp.float32),
            dma((halves, parts, 1 << dims)),
            dma((halves, parts, 1 << dims)),
            dma((halves, parts, 1 << dims)),
            dma((halves, parts, 1 << dims)),
            dma((halves, extra)),
            dma((halves, extra)),
            dma((halves, extra)),
            dma((halves, extra)),
        ],
        compiler_params=pltpu.CompilerParams(
            collective_id=0, has_side_effects=True
        ),
    )(
        stream,
        norm_gain.reshape(groups, 1, cols),
        *weights,
        write_weight.T,
        decay_weight.T,
        rate.reshape(1, heads),
    )


def split(v):
    high = v.astype(jnp.bfloat16)
    return high, (v - high.astype(jnp.float32)).astype(jnp.bfloat16)


def state_kernel(
    state_ref, packed_ref, gain_ref, new_ref, gated_ref, flat_ref, held, readout, in_sems, out_sems
):
    total, size, _ = state_ref.shape
    steps = in_sems.shape[0]
    count = total // steps

    def rows_of(step):
        return pl.ds(pl.multiple_of(step * count, count), count)

    def fetch(step):
        rows = rows_of(step)
        return pltpu.make_async_copy(state_ref.at[rows], held.at[rows], in_sems.at[step])

    def store(step):
        rows = rows_of(step)
        return pltpu.make_async_copy(held.at[rows], new_ref.at[rows], out_sems.at[step])

    for step in range(steps):
        fetch(step).start()
    spots = lax.broadcasted_iota(jnp.int32, (4 * count, size), 0) % count

    def diagonal(rows):
        marks = spots[0 : rows.shape[0]]
        return jnp.concatenate(
            [jnp.where(marks == b, rows, jnp.zeros_like(rows)) for b in range(count)], axis=1
        )

    def body(step, carry):
        rows = rows_of(step)

        def columns(first, width=1):
            return packed_ref[rows, first * size : (first + width) * size]

        key_high, key_low = split(columns(4))
        query_high, query_low = split(columns(3))
        four = jnp.concatenate([key_high, key_low, query_high, query_low], axis=0)
        strength, factor, overlap = columns(0), columns(1), columns(2)
        left = jnp.concatenate([key_high, key_low, key_high], axis=0)
        left = jnp.concatenate([left, jnp.zeros((size - 3 * count, size), left.dtype)], axis=0)
        left = left.astype(jnp.float32).T.astype(jnp.bfloat16)[:, 0 : 3 * count]
        wide = diagonal(four)
        fetch(step).wait()
        memory = held[rows].reshape(count * size, size).astype(jnp.bfloat16)
        both = jnp.dot(wide, memory, preferred_element_type=jnp.float32)
        recalled = both[0:count] + both[count : 2 * count]
        asked = both[2 * count : 3 * count] + both[3 * count : 4 * count]
        change = strength * (columns(5) - factor * recalled)
        readout[rows, :] = factor * asked + overlap * change
        change_high, change_low = split(change)
        right = diagonal(jnp.concatenate([change_high, change_high, change_low], axis=0))
        outer = jnp.dot(left, right, preferred_element_type=jnp.float32)
        for b in range(count):
            spot = step * count + b
            held[spot] = factor[b : b + 1, :] * held[spot] + outer[:, b * size : (b + 1) * size]
        store(step).start()
        return carry

    lax.fori_loop(0, steps, body, 0)
    read = readout[...]
    scaling = lax.rsqrt(jnp.sum(read * read, axis=1, keepdims=True) / size + EPS)
    gate = packed_ref[:, 6 * size :]
    gated_ref[...] = (
        read * gain_ref[...].astype(jnp.float32) * (gate / (1.0 + jnp.exp(-gate)))
    ).astype(jnp.bfloat16)
    tall = jnp.broadcast_to(scaling, (total, 128))
    if total < 128:
        tall = jnp.concatenate([tall, jnp.zeros((128 - total, 128), jnp.float32)], axis=0)
    flat_ref[...] = tall.T[0:SMALL, 0:total].astype(jnp.bfloat16)
    for step in range(steps):
        store(step).wait()


def state_step(state, packed, head_gain):
    count, size, _ = state.shape
    steps = count // min(16, count)
    anywhere = pl.BlockSpec(memory_space=pl.ANY)
    return pl.pallas_call(
        state_kernel,
        in_specs=[anywhere, VMEM, VMEM],
        out_specs=[anywhere, VMEM, VMEM],
        out_shape=[
            jax.ShapeDtypeStruct(state.shape, state.dtype),
            jax.ShapeDtypeStruct((count, size), jnp.bfloat16),
            jax.ShapeDtypeStruct((SMALL, count), jnp.bfloat16),
        ],
        scratch_shapes=[
            pltpu.VMEM(state.shape, state.dtype),
            pltpu.VMEM((count, size), jnp.float32),
            pltpu.SemaphoreType.DMA((steps,)),
            pltpu.SemaphoreType.DMA((steps,)),
        ],
    )(state, packed, head_gain.reshape(1, size))


def output_kernel(
    heads,
    groups,
    stream_ref,
    gated_ref,
    scaling_ref,
    weight_hbm,
    out_ref,
    weight_ref,
    weight_sem,
    all_gated,
    all_scaling,
    columns,
    held,
    core_out,
    core_in,
    hop_out,
    hop_in,
    gated_send,
    gated_recv,
    scaling_send,
    scaling_recv,
    core_send,
    core_recv,
    hop_send,
    hop_recv,
):
    me = lax.axis_index("tp")
    place = me % heads
    group = me // heads
    rows, cols = stream_ref.shape
    batch = all_gated.shape[0]
    group_rows = batch // groups
    dims = heads.bit_length() - 2
    chips = 1 << dims
    sibling = flip(me, (0,))
    neighbours = [flip(me, (bit,)) for bit in range(1, dims + 1)]
    others = [place + heads * ((group + j) % groups) for j in range(1, groups)]
    weight_copy = pltpu.make_async_copy(weight_hbm, weight_ref, weight_sem)
    weight_copy.start()
    enter([sibling] + neighbours + others)
    own_rows = pl.ds(pl.multiple_of(group * group_rows, group_rows), group_rows)
    copies = []
    arriving = []
    for j in range(1, groups):
        for source, target, send, recv in (
            (gated_ref, all_gated.at[own_rows], gated_send, gated_recv),
            (scaling_ref, all_scaling.at[group], scaling_send, scaling_recv),
        ):
            copy = remote(source, target, send.at[j - 1], recv.at[j - 1], others[j - 1])
            copy.start()
            copies.append(copy)
    all_gated[own_rows, :] = gated_ref[...]
    all_scaling[group] = scaling_ref[...]
    for copy in copies:
        copy.wait_recv()
    weight_copy.wait()
    wide = max(group_rows, 128)
    for g in range(groups):
        flat = all_scaling[g].astype(jnp.float32)
        if wide > group_rows:
            flat = jnp.concatenate(
                [flat, jnp.zeros((SMALL, wide - group_rows), jnp.float32)], axis=1
            )
        flat = jnp.concatenate([flat, jnp.zeros((128 - SMALL, wide), jnp.float32)], axis=0)
        columns[g * group_rows : (g + 1) * group_rows, :] = flat.T[0:group_rows]

    def relative(owner, mask):
        bits = tuple(bit for bit in range(1, dims + 1) if mask >> (bit - 1) & 1)
        begin = flip(owner, bits) * rows
        return pl.ds(pl.multiple_of(begin, rows), rows)

    def head_rows(owner, masks):
        picks = [relative(owner, mask) for mask in masks]
        left = jnp.concatenate([all_gated[pick, :] for pick in picks], axis=0)
        scale = jnp.concatenate([columns[pick, 0:1] for pick in picks], axis=0)
        product = lax.dot_general(
            left, weight_ref[...], (((1,), (1,)), ((), ())), preferred_element_type=jnp.float32
        )
        return product * scale

    core_copies = [
        remote(
            core_out.at[mask], core_in.at[mask], core_send.at[mask], core_recv.at[mask], sibling
        )
        for mask in range(chips)
    ]
    batch_of = min(4, chips)
    sweep = list(range(chips - 1, -1, -1))
    for first in range(0, chips, batch_of):
        masks = sweep[first : first + batch_of]
        product = head_rows(flip(place, (0,)), masks).astype(jnp.bfloat16)
        for i, mask in enumerate(masks):
            core_out[mask] = product[i * rows : (i + 1) * rows]
            core_copies[mask].start()
    for first in range(0, chips, batch_of):
        masks = sweep[first : first + batch_of]
        product = head_rows(place, masks)
        for i, mask in enumerate(masks):
            held[mask] = product[i * rows : (i + 1) * rows]

    parts = parts_of(cols, dims)
    hops = []
    waiting = [[] for _ in range(dims)]

    def cross(step, p, mask):
        (start, width), order = parts[p]
        if step == dims or not mask >> (order[step] - 1) & 1:
            return
        span = pl.ds(start, width)
        landed = mask - (1 << (order[step] - 1))
        hop_out[step, landed, :, span] = held[mask, :, span].astype(jnp.bfloat16)
        copy = remote(
            hop_out.at[step, landed, :, span],
            hop_in.at[step, landed, :, span],
            hop_send.at[step, p, landed],
            hop_recv.at[step, p, landed],
            neighbours[order[step] - 1],
        )
        copy.start()
        hops.append(copy)
        waiting[step].append((p, landed, span, copy))

    for mask in sweep:
        core_copies[mask].wait_recv()
        held[mask] += core_in[mask].astype(jnp.float32)
        for p in range(len(parts)):
            cross(0, p, mask)
    for step in range(dims):
        for p, landed, span, copy in waiting[step]:
            copy.wait_recv()
            held[landed, :, span] += hop_in[step, landed, :, span].astype(jnp.float32)
            cross(step + 1, p, landed)
    out_ref[...] = (stream_ref[...].astype(jnp.float32) + held[0]).astype(jnp.bfloat16)
    for copy in copies + core_copies + hops:
        copy.wait_send()


def output(stream, gated, scaling, out_weight, heads, groups):
    rows, cols = stream.shape
    batch = rows * heads
    group_rows, size = gated.shape
    dims = heads.bit_length() - 2
    chips = 1 << dims
    parts = len(parts_of(cols, dims))
    extra = groups - 1
    dma = pltpu.SemaphoreType.DMA
    anywhere = pl.BlockSpec(memory_space=pl.ANY)
    return pl.pallas_call(
        functools.partial(output_kernel, heads, groups),
        in_specs=[VMEM] * 3 + [anywhere],
        out_specs=VMEM,
        out_shape=jax.ShapeDtypeStruct(stream.shape, stream.dtype),
        scratch_shapes=[
            pltpu.VMEM(out_weight.shape, out_weight.dtype),
            dma(()),
            pltpu.VMEM((batch, size), jnp.bfloat16),
            pltpu.VMEM((groups, SMALL, group_rows), jnp.bfloat16),
            pltpu.VMEM((batch, 128), jnp.float32),
            pltpu.VMEM((chips, rows, cols), jnp.float32),
            pltpu.VMEM((chips, rows, cols), jnp.bfloat16),
            pltpu.VMEM((chips, rows, cols), jnp.bfloat16),
            pltpu.VMEM((dims, chips, rows, cols), jnp.bfloat16),
            pltpu.VMEM((dims, chips, rows, cols), jnp.bfloat16),
            dma((extra,)),
            dma((extra,)),
            dma((extra,)),
            dma((extra,)),
            dma((chips,)),
            dma((chips,)),
            dma((dims, parts, chips)),
            dma((dims, parts, chips)),
        ],
        compiler_params=pltpu.CompilerParams(
            collective_id=1, has_side_effects=True
        ),
    )(stream, gated, scaling, out_weight)


def per_device(
    stream,
    norm_gain,
    query_weight,
    key_weight,
    value_weight,
    gate_weight,
    write_weight,
    decay_weight,
    decay_rate,
    head_gain,
    out_weight,
    state,
):
    heads = decay_rate.shape[0]
    groups = lax.axis_size("tp") // heads
    weights = (query_weight, key_weight, value_weight, gate_weight)
    packed = project(
        stream, norm_gain, weights, write_weight, decay_weight, decay_rate, heads, groups
    )
    updated, gated, scaling = state_step(state, packed, head_gain)
    result = output(stream, gated, scaling, out_weight, heads, groups)
    return (result, updated)


def solution(mesh):
    placed = (
        P("tp", None),
        P(),
        P("tp", None),
        P("tp", None),
        P("tp", None),
        P("tp", None),
        P(),
        P(),
        P(),
        P(),
        P("tp", None),
        P("tp", None, None),
    )
    return jax.shard_map(
        per_device,
        mesh=mesh,
        in_specs=placed,
        out_specs=(P("tp", None), P("tp", None, None)),
        check_vma=False,
    )
```

```python
import functools

import jax
import jax.numpy as jnp
from jax import lax
from jax.experimental import pallas as pl
from jax.experimental.pallas import tpu as pltpu
from jax.sharding import PartitionSpec as P

EPS = 1e-06
MESH = pl.DeviceIdType.MESH
VMEM = pl.BlockSpec(memory_space=pltpu.VMEM)
SMALL = 16


def flip(me, bits):
    other = me
    for bit in bits:
        other = other + (1 - 2 * ((me // (1 << bit)) % 2)) * (1 << bit)
    return other


def parts_of(cols, dims):
    tiles = cols // 128
    count = max(1, min(dims, tiles))
    cuts = [tiles * i // count * 128 for i in range(count + 1)]
    ranges = [(cuts[i], cuts[i + 1] - cuts[i]) for i in range(count)]
    orders = [[1 + (i + j) % dims for j in range(dims)] for i in range(count)]
    return list(zip(ranges, orders))


def masks_of(order):
    sets = [((), -1)]
    for step in range(len(order)):
        sets = sets + [(bits + (order[step],), step) for bits, _ in sets]
    return sets


def key_of(bits):
    return sum(1 << (bit - 1) for bit in bits)


def enter(devices):
    barrier = pltpu.get_barrier_semaphore()
    for device in devices:
        pl.semaphore_signal(barrier, inc=1, device_id=(device,), device_id_type=MESH)
    pl.semaphore_wait(barrier, len(devices))


def remote(source, target, send_sem, recv_sem, device):
    return pltpu.make_async_remote_copy(
        src_ref=source,
        dst_ref=target,
        send_sem=send_sem,
        recv_sem=recv_sem,
        device_id=(device,),
        device_id_type=MESH,
    )


def project_kernel(
    heads,
    groups,
    stream_ref,
    gain_ref,
    query_w,
    key_w,
    value_w,
    gate_w,
    write_w,
    decay_w,
    rate_ref,
    packed_out,
    gathered,
    weights,
    write_t,
    decay_t,
    gains,
    local_sems,
    partial,
    sent,
    received,
    small_sent,
    small_received,
    turned,
    ici_send,
    ici_recv,
    core_send,
    core_recv,
    group_send,
    group_recv,
    small_send,
    small_recv,
):
    me = lax.axis_index("tp")
    place = me % heads
    group = me // heads
    rows, cols = stream_ref.shape
    batch = gathered.shape[0]
    group_rows = batch // groups
    dims = heads.bit_length() - 2
    sibling = flip(me, (0,))
    neighbours = [flip(me, (bit,)) for bit in range(1, dims + 1)]
    others = [place + heads * ((group + j) % groups) for j in range(1, groups)]
    size = query_w.shape[1]
    own_cols = pl.ds(pl.multiple_of(group * cols, cols), cols)
    fetches = [
        pltpu.make_async_copy(
            weight, weights.at[:, i * size : (i + 1) * size], local_sems.at[i]
        )
        for i, weight in enumerate((query_w, key_w, value_w, gate_w))
    ] + [
        pltpu.make_async_copy(source.at[:, own_cols], target, local_sems.at[4 + i])
        for i, (source, target) in enumerate(((write_w, write_t), (decay_w, decay_t)))
    ]
    for fetch in fetches:
        fetch.start()
    enter([sibling] + neighbours + others)

    halves = 2 if rows % 32 == 0 and group_rows % rows == 0 else 1
    part_rows = rows // halves
    half_batch = batch // halves
    ranges = parts_of(cols, dims)

    def half_rows(h, device_place):
        begin = h * half_batch + device_place * part_rows
        return pl.ds(pl.multiple_of(begin, part_rows), part_rows)

    def block(h, device_place, part):
        return gathered.at[half_rows(h, device_place), pl.ds(part[0][0], part[0][1])]

    sends = []
    core_copies = [[] for _ in range(halves)]

    def pass_on(h, p, part, bits, step):
        order = part[1]
        origin = flip(place, bits)
        target = block(h, origin, part)
        if bits:
            source = target
        else:
            source = stream_ref.at[
                pl.ds(h * part_rows, part_rows), pl.ds(part[0][0], part[0][1])
            ]
        for later in range(step + 1, dims):
            landed = key_of(bits + (order[later],))
            copy = remote(
                source,
                target,
                ici_send.at[h, p, landed],
                ici_recv.at[h, p, landed],
                flip(me, (order[later],)),
            )
            copy.start()
            sends.append(copy)
        own = key_of(bits)
        copy = remote(source, target, core_send.at[h, p, own], core_recv.at[h, p, own], sibling)
        copy.start()
        core_copies[h].append(copy)

    def begin(h):
        for p, part in enumerate(ranges):
            pass_on(h, p, part, (), -1)

    def relay(h, index):
        for p, part in enumerate(ranges):
            bits, step = masks_of(part[1])[index]
            landed = key_of(bits)
            target = block(h, flip(place, bits), part)
            remote(
                target, target, ici_send.at[h, p, landed], ici_recv.at[h, p, landed], sibling
            ).wait_recv()
            pass_on(h, p, part, bits, step)

    early = 1
    begin(0)
    for h in range(halves):
        gathered[half_rows(h, place), :] = stream_ref[h * part_rows : (h + 1) * part_rows, :]
    relay(0, 1)
    for h in range(1, halves):
        begin(h)
    for index in range(2, 1 << dims):
        relay(0, index)
    for h in range(1, halves):
        for index in range(1, early):
            relay(h, index)
    for copy in core_copies[0]:
        copy.wait_recv()

    gains[...] = gain_ref[...].astype(jnp.float32)
    gain = jnp.concatenate(
        [gains[pl.ds(group * (cols // 128) + i, 1), :] for i in range(cols // 128)], axis=1
    )
    for fetch in fetches:
        fetch.wait()

    def project(begin, count, at):
        x = gathered[pl.ds(begin, count), :].astype(jnp.float32)
        gained = (x * gain).astype(jnp.bfloat16)
        partial[pl.ds(at, count), :] = jnp.dot(
            gained, weights[...], preferred_element_type=jnp.float32
        )
        mine = lax.broadcasted_iota(jnp.int32, (count, heads), 1) == place
        pre = [
            jnp.sum(
                jnp.where(
                    mine,
                    lax.dot_general(
                        gained,
                        w[...],
                        (((1,), (1,)), ((), ())),
                        preferred_element_type=jnp.float32,
                    ),
                    0.0,
                ),
                axis=1,
                keepdims=True,
            )
            for w in (write_t, decay_t)
        ]
        squares = jnp.sum(x * x, axis=1, keepdims=True)
        lane = lax.broadcasted_iota(jnp.int32, (count, 128), 1)
        return jnp.where(
            lane == 0, pre[0], jnp.where(lane == 1, pre[1], jnp.where(lane == 2, squares, 0.0))
        )

    copies = []
    wide = max(group_rows, 128)
    count = group_rows // halves

    def half_of(h, target_group):
        begin = h * half_batch + target_group * count
        return pl.multiple_of(begin, count)

    for h in range(halves):
        if h:
            for index in range(early, 1 << dims):
                relay(h, index)
            for copy in core_copies[h]:
                copy.wait_recv()
        for j in range(1, groups):
            spot = slice(h * count, (h + 1) * count)
            side = project(half_of(h, (group + j) % groups), count, 0)
            sent[j - 1, spot] = partial[0:count].astype(jnp.bfloat16)
            turned[spot] = side
            routes = [(sent.at[j - 1, spot], received.at[j - 1, spot], group_send, group_recv)]
            flat = turned[...].T
            small_sent[j - 1, :, spot] = flat[0:SMALL, spot].astype(jnp.bfloat16)
            routes.append(
                (
                    small_sent.at[j - 1, :, spot],
                    small_received.at[j - 1, :, spot],
                    small_send,
                    small_recv,
                )
            )
            for source, target, send, recv in routes:
                copy = remote(
                    source, target, send.at[h, j - 1], recv.at[h, j - 1], others[j - 1]
                )
                copy.start()
                copies.append(copy)
    for h in range(halves):
        turned[h * count : (h + 1) * count] = project(half_of(h, group), count, h * count)
    total = partial[...]
    flat = turned[...].T[0:SMALL, :]
    for copy in copies:
        copy.wait_recv()
    for j in range(1, groups):
        total = total + received[j - 1].astype(jnp.float32)
    small_total = flat[:, 0:group_rows]
    for j in range(1, groups):
        small_total = small_total + small_received[j - 1].astype(jnp.float32)
    turned_back = jnp.concatenate(
        [small_total, jnp.zeros((SMALL, wide - group_rows), jnp.float32)], axis=1
    ) if wide > group_rows else small_total
    side = jnp.concatenate(
        [turned_back, jnp.zeros((128 - SMALL, wide), jnp.float32)], axis=0
    ).T[0:group_rows]
    scale = lax.rsqrt(side[:, 2:3] / (cols * groups) + EPS)

    def rounded(v):
        return v.astype(jnp.bfloat16).astype(jnp.float32)

    projected = rounded(total * scale)
    query = projected[:, :size]
    key = projected[:, size : 2 * size]
    query = query * lax.rsqrt(jnp.sum(query * query, axis=1, keepdims=True) + EPS) * size**-0.5
    key = key * lax.rsqrt(jnp.sum(key * key, axis=1, keepdims=True) + EPS)
    pre = rounded(side * scale)
    strength = jax.nn.sigmoid(pre[:, 0:1])
    mine = lax.broadcasted_iota(jnp.int32, rate_ref.shape, 1) == place
    rate = jnp.sum(jnp.where(mine, rate_ref[...], 0.0), axis=1, keepdims=True)
    decay = pre[:, 1:2]
    softplus = jnp.maximum(decay, 0.0) + jnp.log(1.0 + jnp.exp(-jnp.abs(decay)))
    factor = jnp.exp(-rate * softplus)
    overlap = jnp.sum(query * key, axis=1, keepdims=True)
    results = [jnp.broadcast_to(v, (group_rows, size)) for v in (strength, factor, overlap)]
    results += [query, key, projected[:, 2 * size :]]
    for i, v in enumerate(results):
        span = pl.ds(i * size, v.shape[1])
        if halves == 1:
            packed_out[:, span] = v
            continue
        for h in range(halves):
            for q in range(group_rows // rows):
                to, come = q * rows + h * part_rows, h * count + q * part_rows
                packed_out[to : to + part_rows, span] = v[come : come + part_rows]
    for copy in sends + sum(core_copies, []) + copies:
        copy.wait_send()


def project(stream, norm_gain, weights, write_weight, decay_weight, rate, heads, groups):
    rows, cols = stream.shape
    batch = rows * heads
    group_rows = batch // groups
    size = weights[0].shape[1]
    dims = heads.bit_length() - 2
    parts = len(parts_of(cols, dims))
    extra = groups - 1
    halves = 2
    dma = pltpu.SemaphoreType.DMA
    anywhere = pl.BlockSpec(memory_space=pl.ANY)
    return pl.pallas_call(
        functools.partial(project_kernel, heads, groups),
        in_specs=[VMEM] * 2 + [anywhere] * 6 + [VMEM],
        out_specs=VMEM,
        out_shape=jax.ShapeDtypeStruct((group_rows, 7 * size), jnp.float32),
        scratch_shapes=[
            pltpu.VMEM((batch, cols), jnp.bfloat16),
            pltpu.VMEM((cols, 4 * size), jnp.bfloat16),
            pltpu.VMEM((heads, cols), jnp.bfloat16),
            pltpu.VMEM((heads, cols), jnp.bfloat16),
            pltpu.VMEM((groups * cols // 128, 128), jnp.float32),
            dma((6,)),
            pltpu.VMEM((group_rows, 4 * size), jnp.float32),
            pltpu.VMEM((extra, group_rows, 4 * size), jnp.bfloat16),
            pltpu.VMEM((extra, group_rows, 4 * size), jnp.bfloat16),
            pltpu.VMEM((extra, SMALL, group_rows), jnp.bfloat16),
            pltpu.VMEM((extra, SMALL, group_rows), jnp.bfloat16),
            pltpu.VMEM((max(group_rows, 128), 128), jnp.float32),
            dma((halves, parts, 1 << dims)),
            dma((halves, parts, 1 << dims)),
            dma((halves, parts, 1 << dims)),
            dma((halves, parts, 1 << dims)),
            dma((halves, extra)),
            dma((halves, extra)),
            dma((halves, extra)),
            dma((halves, extra)),
        ],
        compiler_params=pltpu.CompilerParams(
            collective_id=0, has_side_effects=True
        ),
    )(
        stream,
        norm_gain.reshape(groups * cols // 128, 128),
        *weights,
        write_weight.T,
        decay_weight.T,
        rate.reshape(1, heads),
    )


def split(v):
    high = v.astype(jnp.bfloat16)
    return high, (v - high.astype(jnp.float32)).astype(jnp.bfloat16)


def state_kernel(
    state_ref, packed_ref, gain_ref, new_ref, gated_ref, flat_ref, held, readout, in_sems, out_sems
):
    total, size, _ = state_ref.shape
    steps = in_sems.shape[0]
    count = total // steps

    def rows_of(step):
        return pl.ds(pl.multiple_of(step * count, count), count)

    def fetch(step):
        rows = rows_of(step)
        return pltpu.make_async_copy(state_ref.at[rows], held.at[rows], in_sems.at[step])

    def store(step):
        rows = rows_of(step)
        return pltpu.make_async_copy(held.at[rows], new_ref.at[rows], out_sems.at[step])

    for step in range(steps):
        fetch(step).start()
    spots = lax.broadcasted_iota(jnp.int32, (4 * count, size), 0) % count

    def diagonal(rows):
        marks = spots[0 : rows.shape[0]]
        return jnp.concatenate(
            [jnp.where(marks == b, rows, jnp.zeros_like(rows)) for b in range(count)], axis=1
        )

    def body(step, carry):
        rows = rows_of(step)

        def columns(first, width=1):
            return packed_ref[rows, first * size : (first + width) * size]

        key_high, key_low = split(columns(4))
        query_high, query_low = split(columns(3))
        four = jnp.concatenate([key_high, key_low, query_high, query_low], axis=0)
        strength, factor, overlap = columns(0), columns(1), columns(2)
        left = jnp.concatenate([key_high, key_low, key_high], axis=0)
        left = jnp.concatenate([left, jnp.zeros((size - 3 * count, size), left.dtype)], axis=0)
        left = left.astype(jnp.float32).T.astype(jnp.bfloat16)[:, 0 : 3 * count]
        wide = diagonal(four)
        fetch(step).wait()
        memory = held[rows].reshape(count * size, size).astype(jnp.bfloat16)
        both = jnp.dot(wide, memory, preferred_element_type=jnp.float32)
        recalled = both[0:count] + both[count : 2 * count]
        asked = both[2 * count : 3 * count] + both[3 * count : 4 * count]
        change = strength * (columns(5) - factor * recalled)
        readout[rows, :] = factor * asked + overlap * change
        change_high, change_low = split(change)
        right = diagonal(jnp.concatenate([change_high, change_high, change_low], axis=0))
        outer = jnp.dot(left, right, preferred_element_type=jnp.float32)
        for b in range(count):
            spot = step * count + b
            held[spot] = factor[b : b + 1, :] * held[spot] + outer[:, b * size : (b + 1) * size]
        store(step).start()
        return carry

    lax.fori_loop(0, steps, body, 0)
    read = readout[...]
    scaling = lax.rsqrt(jnp.sum(read * read, axis=1, keepdims=True) / size + EPS)
    gate = packed_ref[:, 6 * size :]
    gated_ref[...] = (
        read * gain_ref[...].astype(jnp.float32) * (gate / (1.0 + jnp.exp(-gate)))
    ).astype(jnp.bfloat16)
    tall = jnp.broadcast_to(scaling, (total, 128))
    if total < 128:
        tall = jnp.concatenate([tall, jnp.zeros((128 - total, 128), jnp.float32)], axis=0)
    flat_ref[...] = tall.T[0:SMALL, 0:total].astype(jnp.bfloat16)
    for step in range(steps):
        store(step).wait()


def state_step(state, packed, head_gain):
    count, size, _ = state.shape
    steps = count // min(16, count)
    anywhere = pl.BlockSpec(memory_space=pl.ANY)
    return pl.pallas_call(
        state_kernel,
        in_specs=[anywhere, VMEM, VMEM],
        out_specs=[anywhere, VMEM, VMEM],
        out_shape=[
            jax.ShapeDtypeStruct(state.shape, state.dtype),
            jax.ShapeDtypeStruct((count, size), jnp.bfloat16),
            jax.ShapeDtypeStruct((SMALL, count), jnp.bfloat16),
        ],
        scratch_shapes=[
            pltpu.VMEM(state.shape, state.dtype),
            pltpu.VMEM((count, size), jnp.float32),
            pltpu.SemaphoreType.DMA((steps,)),
            pltpu.SemaphoreType.DMA((steps,)),
        ],
    )(state, packed, head_gain.reshape(1, size))


def output_kernel(
    heads,
    groups,
    stream_ref,
    gated_ref,
    scaling_ref,
    weight_hbm,
    out_ref,
    weight_ref,
    weight_sem,
    all_gated,
    all_scaling,
    columns,
    held,
    core_out,
    core_in,
    hop_out,
    hop_in,
    gated_send,
    gated_recv,
    scaling_send,
    scaling_recv,
    core_send,
    core_recv,
    hop_send,
    hop_recv,
):
    me = lax.axis_index("tp")
    place = me % heads
    group = me // heads
    rows, cols = stream_ref.shape
    batch = all_gated.shape[0]
    group_rows = batch // groups
    dims = heads.bit_length() - 2
    chips = 1 << dims
    sibling = flip(me, (0,))
    neighbours = [flip(me, (bit,)) for bit in range(1, dims + 1)]
    others = [place + heads * ((group + j) % groups) for j in range(1, groups)]
    weight_copy = pltpu.make_async_copy(weight_hbm, weight_ref, weight_sem)
    weight_copy.start()
    enter([sibling] + neighbours + others)
    own_rows = pl.ds(pl.multiple_of(group * group_rows, group_rows), group_rows)
    copies = []
    arriving = []
    for j in range(1, groups):
        for source, target, send, recv in (
            (gated_ref, all_gated.at[own_rows], gated_send, gated_recv),
            (scaling_ref, all_scaling.at[group], scaling_send, scaling_recv),
        ):
            copy = remote(source, target, send.at[j - 1], recv.at[j - 1], others[j - 1])
            copy.start()
            copies.append(copy)
    all_gated[own_rows, :] = gated_ref[...]
    all_scaling[group] = scaling_ref[...]
    for copy in copies:
        copy.wait_recv()
    weight_copy.wait()
    wide = max(group_rows, 128)
    for g in range(groups):
        flat = all_scaling[g].astype(jnp.float32)
        if wide > group_rows:
            flat = jnp.concatenate(
                [flat, jnp.zeros((SMALL, wide - group_rows), jnp.float32)], axis=1
            )
        flat = jnp.concatenate([flat, jnp.zeros((128 - SMALL, wide), jnp.float32)], axis=0)
        columns[g * group_rows : (g + 1) * group_rows, :] = flat.T[0:group_rows]

    def relative(owner, mask):
        bits = tuple(bit for bit in range(1, dims + 1) if mask >> (bit - 1) & 1)
        begin = flip(owner, bits) * rows
        return pl.ds(pl.multiple_of(begin, rows), rows)

    def head_rows(owner, masks):
        picks = [relative(owner, mask) for mask in masks]
        left = jnp.concatenate([all_gated[pick, :] for pick in picks], axis=0)
        scale = jnp.concatenate([columns[pick, 0:1] for pick in picks], axis=0)
        product = lax.dot_general(
            left, weight_ref[...], (((1,), (1,)), ((), ())), preferred_element_type=jnp.float32
        )
        return product * scale

    core_copies = [
        remote(
            core_out.at[mask], core_in.at[mask], core_send.at[mask], core_recv.at[mask], sibling
        )
        for mask in range(chips)
    ]
    batch_of = min(4, chips)
    sweep = list(range(chips - 1, -1, -1))
    for first in range(0, chips, batch_of):
        masks = sweep[first : first + batch_of]
        product = head_rows(flip(place, (0,)), masks).astype(jnp.bfloat16)
        for i, mask in enumerate(masks):
            core_out[mask] = product[i * rows : (i + 1) * rows]
            core_copies[mask].start()
    for first in range(0, chips, batch_of):
        masks = sweep[first : first + batch_of]
        product = head_rows(place, masks)
        for i, mask in enumerate(masks):
            held[mask] = product[i * rows : (i + 1) * rows]

    parts = parts_of(cols, dims)
    hops = []
    waiting = [[] for _ in range(dims)]

    def cross(step, p, mask):
        (start, width), order = parts[p]
        if step == dims or not mask >> (order[step] - 1) & 1:
            return
        span = pl.ds(start, width)
        landed = mask - (1 << (order[step] - 1))
        hop_out[step, landed, :, span] = held[mask, :, span].astype(jnp.bfloat16)
        copy = remote(
            hop_out.at[step, landed, :, span],
            hop_in.at[step, landed, :, span],
            hop_send.at[step, p, landed],
            hop_recv.at[step, p, landed],
            neighbours[order[step] - 1],
        )
        copy.start()
        hops.append(copy)
        waiting[step].append((p, landed, span, copy))

    for mask in sweep:
        core_copies[mask].wait_recv()
        held[mask] += core_in[mask].astype(jnp.float32)
        for p in range(len(parts)):
            cross(0, p, mask)
    for step in range(dims):
        for p, landed, span, copy in waiting[step]:
            copy.wait_recv()
            held[landed, :, span] += hop_in[step, landed, :, span].astype(jnp.float32)
            cross(step + 1, p, landed)
    out_ref[...] = (stream_ref[...].astype(jnp.float32) + held[0]).astype(jnp.bfloat16)
    for copy in copies + core_copies + hops:
        copy.wait_send()


def output(stream, gated, scaling, out_weight, heads, groups):
    rows, cols = stream.shape
    batch = rows * heads
    group_rows, size = gated.shape
    dims = heads.bit_length() - 2
    chips = 1 << dims
    parts = len(parts_of(cols, dims))
    extra = groups - 1
    dma = pltpu.SemaphoreType.DMA
    anywhere = pl.BlockSpec(memory_space=pl.ANY)
    return pl.pallas_call(
        functools.partial(output_kernel, heads, groups),
        in_specs=[VMEM] * 3 + [anywhere],
        out_specs=VMEM,
        out_shape=jax.ShapeDtypeStruct(stream.shape, stream.dtype),
        scratch_shapes=[
            pltpu.VMEM(out_weight.shape, out_weight.dtype),
            dma(()),
            pltpu.VMEM((batch, size), jnp.bfloat16),
            pltpu.VMEM((groups, SMALL, group_rows), jnp.bfloat16),
            pltpu.VMEM((batch, 128), jnp.float32),
            pltpu.VMEM((chips, rows, cols), jnp.float32),
            pltpu.VMEM((chips, rows, cols), jnp.bfloat16),
            pltpu.VMEM((chips, rows, cols), jnp.bfloat16),
            pltpu.VMEM((dims, chips, rows, cols), jnp.bfloat16),
            pltpu.VMEM((dims, chips, rows, cols), jnp.bfloat16),
            dma((extra,)),
            dma((extra,)),
            dma((extra,)),
            dma((extra,)),
            dma((chips,)),
            dma((chips,)),
            dma((dims, parts, chips)),
            dma((dims, parts, chips)),
        ],
        compiler_params=pltpu.CompilerParams(
            collective_id=1, has_side_effects=True
        ),
    )(stream, gated, scaling, out_weight)


def per_device(
    stream,
    norm_gain,
    query_weight,
    key_weight,
    value_weight,
    gate_weight,
    write_weight,
    decay_weight,
    decay_rate,
    head_gain,
    out_weight,
    state,
):
    heads = decay_rate.shape[0]
    groups = lax.axis_size("tp") // heads
    weights = (query_weight, key_weight, value_weight, gate_weight)
    packed = project(
        stream, norm_gain, weights, write_weight, decay_weight, decay_rate, heads, groups
    )
    updated, gated, scaling = state_step(state, packed, head_gain)
    result = output(stream, gated, scaling, out_weight, heads, groups)
    return (result, updated)


def solution(mesh):
    placed = (
        P("tp", None),
        P(),
        P("tp", None),
        P("tp", None),
        P("tp", None),
        P("tp", None),
        P(),
        P(),
        P(),
        P(),
        P("tp", None),
        P("tp", None, None),
    )
    return jax.shard_map(
        per_device,
        mesh=mesh,
        in_specs=placed,
        out_specs=(P("tp", None), P("tp", None, None)),
        check_vma=False,
    )
```

```python
import functools

import jax
import jax.numpy as jnp
from jax import lax
from jax.experimental import pallas as pl
from jax.experimental.pallas import tpu as pltpu
from jax.sharding import PartitionSpec as P

EPS = 1e-06
MESH = pl.DeviceIdType.MESH
VMEM = pl.BlockSpec(memory_space=pltpu.VMEM)
SMALL = 16


def flip(me, bits):
    other = me
    for bit in bits:
        other = other + (1 - 2 * ((me // (1 << bit)) % 2)) * (1 << bit)
    return other


def parts_of(cols, dims):
    tiles = cols // 128
    count = max(1, min(dims, tiles))
    cuts = [tiles * i // count * 128 for i in range(count + 1)]
    ranges = [(cuts[i], cuts[i + 1] - cuts[i]) for i in range(count)]
    orders = [[1 + (i + j) % dims for j in range(dims)] for i in range(count)]
    return list(zip(ranges, orders))


def masks_of(order):
    sets = [((), -1)]
    for step in range(len(order)):
        sets = sets + [(bits + (order[step],), step) for bits, _ in sets]
    return sets


def key_of(bits):
    return sum(1 << (bit - 1) for bit in bits)


def enter(devices):
    barrier = pltpu.get_barrier_semaphore()
    for device in devices:
        pl.semaphore_signal(barrier, inc=1, device_id=(device,), device_id_type=MESH)
    pl.semaphore_wait(barrier, len(devices))


def remote(source, target, send_sem, recv_sem, device):
    return pltpu.make_async_remote_copy(
        src_ref=source,
        dst_ref=target,
        send_sem=send_sem,
        recv_sem=recv_sem,
        device_id=(device,),
        device_id_type=MESH,
    )


def project_kernel(
    heads,
    groups,
    stream_ref,
    gain_ref,
    query_w,
    key_w,
    value_w,
    gate_w,
    write_w,
    decay_w,
    rate_ref,
    packed_out,
    gathered,
    weights,
    write_t,
    decay_t,
    gains,
    local_sems,
    partial,
    sent,
    received,
    small_sent,
    small_received,
    turned,
    ici_send,
    ici_recv,
    core_send,
    core_recv,
    group_send,
    group_recv,
    small_send,
    small_recv,
):
    me = lax.axis_index("tp")
    place = me % heads
    group = me // heads
    rows, cols = stream_ref.shape
    batch = gathered.shape[0]
    group_rows = batch // groups
    dims = heads.bit_length() - 2
    sibling = flip(me, (0,))
    neighbours = [flip(me, (bit,)) for bit in range(1, dims + 1)]
    others = [place + heads * ((group + j) % groups) for j in range(1, groups)]
    size = query_w.shape[1]
    own_cols = pl.ds(pl.multiple_of(group * cols, cols), cols)
    fetches = [
        pltpu.make_async_copy(
            weight, weights.at[:, i * size : (i + 1) * size], local_sems.at[i]
        )
        for i, weight in enumerate((query_w, key_w, value_w, gate_w))
    ] + [
        pltpu.make_async_copy(source.at[:, own_cols], target, local_sems.at[4 + i])
        for i, (source, target) in enumerate(((write_w, write_t), (decay_w, decay_t)))
    ]
    for fetch in fetches:
        fetch.start()
    enter([sibling] + neighbours + others)

    halves = 2 if rows % 32 == 0 and group_rows % rows == 0 else 1
    part_rows = rows // halves
    half_batch = batch // halves
    ranges = parts_of(cols, dims)

    def half_rows(h, device_place):
        begin = h * half_batch + device_place * part_rows
        return pl.ds(pl.multiple_of(begin, part_rows), part_rows)

    def block(h, device_place, part):
        return gathered.at[half_rows(h, device_place), pl.ds(part[0][0], part[0][1])]

    sends = []
    core_copies = [[] for _ in range(halves)]

    def pass_on(h, p, part, bits, step):
        order = part[1]
        origin = flip(place, bits)
        target = block(h, origin, part)
        if bits:
            source = target
        else:
            source = stream_ref.at[
                pl.ds(h * part_rows, part_rows), pl.ds(part[0][0], part[0][1])
            ]
        for later in range(step + 1, dims):
            landed = key_of(bits + (order[later],))
            copy = remote(
                source,
                target,
                ici_send.at[h, p, landed],
                ici_recv.at[h, p, landed],
                flip(me, (order[later],)),
            )
            copy.start()
            sends.append(copy)
        own = key_of(bits)
        copy = remote(source, target, core_send.at[h, p, own], core_recv.at[h, p, own], sibling)
        copy.start()
        core_copies[h].append(copy)

    def begin(h):
        for p, part in enumerate(ranges):
            pass_on(h, p, part, (), -1)

    def relay(h, index):
        for p, part in enumerate(ranges):
            bits, step = masks_of(part[1])[index]
            landed = key_of(bits)
            target = block(h, flip(place, bits), part)
            remote(
                target, target, ici_send.at[h, p, landed], ici_recv.at[h, p, landed], sibling
            ).wait_recv()
            pass_on(h, p, part, bits, step)

    early = max(2, 1 << (dims - 1))
    begin(0)
    for h in range(halves):
        gathered[half_rows(h, place), :] = stream_ref[h * part_rows : (h + 1) * part_rows, :]
    relay(0, 1)
    for h in range(1, halves):
        begin(h)
    for index in range(2, 1 << dims):
        relay(0, index)
    for h in range(1, halves):
        for index in range(1, early):
            relay(h, index)
    for copy in core_copies[0]:
        copy.wait_recv()

    gains[...] = gain_ref[...].astype(jnp.float32)
    gain = jnp.concatenate(
        [gains[pl.ds(group * (cols // 128) + i, 1), :] for i in range(cols // 128)], axis=1
    )
    for fetch in fetches:
        fetch.wait()

    def project(begin, count, at):
        x = gathered[pl.ds(begin, count), :].astype(jnp.float32)
        gained = (x * gain).astype(jnp.bfloat16)
        partial[pl.ds(at, count), :] = jnp.dot(
            gained, weights[...], preferred_element_type=jnp.float32
        )
        mine = lax.broadcasted_iota(jnp.int32, (count, heads), 1) == place
        pre = [
            jnp.sum(
                jnp.where(
                    mine,
                    lax.dot_general(
                        gained,
                        w[...],
                        (((1,), (1,)), ((), ())),
                        preferred_element_type=jnp.float32,
                    ),
                    0.0,
                ),
                axis=1,
                keepdims=True,
            )
            for w in (write_t, decay_t)
        ]
        squares = jnp.sum(x * x, axis=1, keepdims=True)
        lane = lax.broadcasted_iota(jnp.int32, (count, 128), 1)
        return jnp.where(
            lane == 0, pre[0], jnp.where(lane == 1, pre[1], jnp.where(lane == 2, squares, 0.0))
        )

    copies = []
    wide = max(group_rows, 128)
    count = group_rows // halves

    def half_of(h, target_group):
        begin = h * half_batch + target_group * count
        return pl.multiple_of(begin, count)

    for h in range(halves):
        if h:
            for index in range(early, 1 << dims):
                relay(h, index)
            for copy in core_copies[h]:
                copy.wait_recv()
        for j in range(1, groups):
            spot = slice(h * count, (h + 1) * count)
            side = project(half_of(h, (group + j) % groups), count, 0)
            sent[j - 1, spot] = partial[0:count].astype(jnp.bfloat16)
            turned[spot] = side
            routes = [(sent.at[j - 1, spot], received.at[j - 1, spot], group_send, group_recv)]
            flat = turned[...].T
            small_sent[j - 1, :, spot] = flat[0:SMALL, spot].astype(jnp.bfloat16)
            routes.append(
                (
                    small_sent.at[j - 1, :, spot],
                    small_received.at[j - 1, :, spot],
                    small_send,
                    small_recv,
                )
            )
            for source, target, send, recv in routes:
                copy = remote(
                    source, target, send.at[h, j - 1], recv.at[h, j - 1], others[j - 1]
                )
                copy.start()
                copies.append(copy)
    for h in range(halves):
        turned[h * count : (h + 1) * count] = project(half_of(h, group), count, h * count)
    total = partial[...]
    flat = turned[...].T[0:SMALL, :]
    for copy in copies:
        copy.wait_recv()
    for j in range(1, groups):
        total = total + received[j - 1].astype(jnp.float32)
    small_total = flat[:, 0:group_rows]
    for j in range(1, groups):
        small_total = small_total + small_received[j - 1].astype(jnp.float32)
    turned_back = jnp.concatenate(
        [small_total, jnp.zeros((SMALL, wide - group_rows), jnp.float32)], axis=1
    ) if wide > group_rows else small_total
    side = jnp.concatenate(
        [turned_back, jnp.zeros((128 - SMALL, wide), jnp.float32)], axis=0
    ).T[0:group_rows]
    scale = lax.rsqrt(side[:, 2:3] / (cols * groups) + EPS)

    def rounded(v):
        return v.astype(jnp.bfloat16).astype(jnp.float32)

    projected = rounded(total * scale)
    query = projected[:, :size]
    key = projected[:, size : 2 * size]
    query = query * lax.rsqrt(jnp.sum(query * query, axis=1, keepdims=True) + EPS) * size**-0.5
    key = key * lax.rsqrt(jnp.sum(key * key, axis=1, keepdims=True) + EPS)
    pre = rounded(side * scale)
    strength = jax.nn.sigmoid(pre[:, 0:1])
    mine = lax.broadcasted_iota(jnp.int32, rate_ref.shape, 1) == place
    rate = jnp.sum(jnp.where(mine, rate_ref[...], 0.0), axis=1, keepdims=True)
    decay = pre[:, 1:2]
    softplus = jnp.maximum(decay, 0.0) + jnp.log(1.0 + jnp.exp(-jnp.abs(decay)))
    factor = jnp.exp(-rate * softplus)
    overlap = jnp.sum(query * key, axis=1, keepdims=True)
    results = [jnp.broadcast_to(v, (group_rows, size)) for v in (strength, factor, overlap)]
    results += [query, key, projected[:, 2 * size :]]
    for i, v in enumerate(results):
        span = pl.ds(i * size, v.shape[1])
        if halves == 1:
            packed_out[:, span] = v
            continue
        for h in range(halves):
            for q in range(group_rows // rows):
                to, come = q * rows + h * part_rows, h * count + q * part_rows
                packed_out[to : to + part_rows, span] = v[come : come + part_rows]
    for copy in sends + sum(core_copies, []) + copies:
        copy.wait_send()


def project(stream, norm_gain, weights, write_weight, decay_weight, rate, heads, groups):
    rows, cols = stream.shape
    batch = rows * heads
    group_rows = batch // groups
    size = weights[0].shape[1]
    dims = heads.bit_length() - 2
    parts = len(parts_of(cols, dims))
    extra = groups - 1
    halves = 2
    dma = pltpu.SemaphoreType.DMA
    anywhere = pl.BlockSpec(memory_space=pl.ANY)
    return pl.pallas_call(
        functools.partial(project_kernel, heads, groups),
        in_specs=[VMEM] * 2 + [anywhere] * 6 + [VMEM],
        out_specs=VMEM,
        out_shape=jax.ShapeDtypeStruct((group_rows, 7 * size), jnp.float32),
        scratch_shapes=[
            pltpu.VMEM((batch, cols), jnp.bfloat16),
            pltpu.VMEM((cols, 4 * size), jnp.bfloat16),
            pltpu.VMEM((heads, cols), jnp.bfloat16),
            pltpu.VMEM((heads, cols), jnp.bfloat16),
            pltpu.VMEM((groups * cols // 128, 128), jnp.float32),
            dma((6,)),
            pltpu.VMEM((group_rows, 4 * size), jnp.float32),
            pltpu.VMEM((extra, group_rows, 4 * size), jnp.bfloat16),
            pltpu.VMEM((extra, group_rows, 4 * size), jnp.bfloat16),
            pltpu.VMEM((extra, SMALL, group_rows), jnp.bfloat16),
            pltpu.VMEM((extra, SMALL, group_rows), jnp.bfloat16),
            pltpu.VMEM((max(group_rows, 128), 128), jnp.float32),
            dma((halves, parts, 1 << dims)),
            dma((halves, parts, 1 << dims)),
            dma((halves, parts, 1 << dims)),
            dma((halves, parts, 1 << dims)),
            dma((halves, extra)),
            dma((halves, extra)),
            dma((halves, extra)),
            dma((halves, extra)),
        ],
        compiler_params=pltpu.CompilerParams(
            collective_id=0, has_side_effects=True
        ),
    )(
        stream,
        norm_gain.reshape(groups * cols // 128, 128),
        *weights,
        write_weight.T,
        decay_weight.T,
        rate.reshape(1, heads),
    )


def split(v):
    high = v.astype(jnp.bfloat16)
    return high, (v - high.astype(jnp.float32)).astype(jnp.bfloat16)


def state_kernel(
    state_ref, packed_ref, gain_ref, new_ref, gated_ref, flat_ref, held, readout, in_sems, out_sems
):
    total, size, _ = state_ref.shape
    steps = in_sems.shape[0]
    count = total // steps

    def rows_of(step):
        return pl.ds(pl.multiple_of(step * count, count), count)

    def fetch(step):
        rows = rows_of(step)
        return pltpu.make_async_copy(state_ref.at[rows], held.at[rows], in_sems.at[step])

    def store(step):
        rows = rows_of(step)
        return pltpu.make_async_copy(held.at[rows], new_ref.at[rows], out_sems.at[step])

    for step in range(steps):
        fetch(step).start()
    spots = lax.broadcasted_iota(jnp.int32, (4 * count, size), 0) % count

    def diagonal(rows):
        marks = spots[0 : rows.shape[0]]
        return jnp.concatenate(
            [jnp.where(marks == b, rows, jnp.zeros_like(rows)) for b in range(count)], axis=1
        )

    def body(step, carry):
        rows = rows_of(step)

        def columns(first, width=1):
            return packed_ref[rows, first * size : (first + width) * size]

        key_high, key_low = split(columns(4))
        query_high, query_low = split(columns(3))
        four = jnp.concatenate([key_high, key_low, query_high, query_low], axis=0)
        strength, factor, overlap = columns(0), columns(1), columns(2)
        left = jnp.concatenate([key_high, key_low, key_high], axis=0)
        left = jnp.concatenate([left, jnp.zeros((size - 3 * count, size), left.dtype)], axis=0)
        left = left.astype(jnp.float32).T.astype(jnp.bfloat16)[:, 0 : 3 * count]
        wide = diagonal(four)
        fetch(step).wait()
        memory = held[rows].reshape(count * size, size).astype(jnp.bfloat16)
        both = jnp.dot(wide, memory, preferred_element_type=jnp.float32)
        recalled = both[0:count] + both[count : 2 * count]
        asked = both[2 * count : 3 * count] + both[3 * count : 4 * count]
        change = strength * (columns(5) - factor * recalled)
        readout[rows, :] = factor * asked + overlap * change
        change_high, change_low = split(change)
        right = diagonal(jnp.concatenate([change_high, change_high, change_low], axis=0))
        outer = jnp.dot(left, right, preferred_element_type=jnp.float32)
        for b in range(count):
            spot = step * count + b
            held[spot] = factor[b : b + 1, :] * held[spot] + outer[:, b * size : (b + 1) * size]
        store(step).start()
        return carry

    lax.fori_loop(0, steps, body, 0)
    read = readout[...]
    scaling = lax.rsqrt(jnp.sum(read * read, axis=1, keepdims=True) / size + EPS)
    gate = packed_ref[:, 6 * size :]
    gated_ref[...] = (
        read * gain_ref[...].astype(jnp.float32) * (gate / (1.0 + jnp.exp(-gate)))
    ).astype(jnp.bfloat16)
    tall = jnp.broadcast_to(scaling, (total, 128))
    if total < 128:
        tall = jnp.concatenate([tall, jnp.zeros((128 - total, 128), jnp.float32)], axis=0)
    flat_ref[...] = tall.T[0:SMALL, 0:total].astype(jnp.bfloat16)
    for step in range(steps):
        store(step).wait()


def state_step(state, packed, head_gain):
    count, size, _ = state.shape
    steps = count // min(16, count)
    anywhere = pl.BlockSpec(memory_space=pl.ANY)
    return pl.pallas_call(
        state_kernel,
        in_specs=[anywhere, VMEM, VMEM],
        out_specs=[anywhere, VMEM, VMEM],
        out_shape=[
            jax.ShapeDtypeStruct(state.shape, state.dtype),
            jax.ShapeDtypeStruct((count, size), jnp.bfloat16),
            jax.ShapeDtypeStruct((SMALL, count), jnp.bfloat16),
        ],
        scratch_shapes=[
            pltpu.VMEM(state.shape, state.dtype),
            pltpu.VMEM((count, size), jnp.float32),
            pltpu.SemaphoreType.DMA((steps,)),
            pltpu.SemaphoreType.DMA((steps,)),
        ],
    )(state, packed, head_gain.reshape(1, size))


def output_kernel(
    heads,
    groups,
    stream_ref,
    gated_ref,
    scaling_ref,
    weight_hbm,
    out_ref,
    weight_ref,
    weight_sem,
    all_gated,
    all_scaling,
    columns,
    held,
    core_out,
    core_in,
    hop_out,
    hop_in,
    gated_send,
    gated_recv,
    scaling_send,
    scaling_recv,
    core_send,
    core_recv,
    hop_send,
    hop_recv,
):
    me = lax.axis_index("tp")
    place = me % heads
    group = me // heads
    rows, cols = stream_ref.shape
    batch = all_gated.shape[0]
    group_rows = batch // groups
    dims = heads.bit_length() - 2
    chips = 1 << dims
    sibling = flip(me, (0,))
    neighbours = [flip(me, (bit,)) for bit in range(1, dims + 1)]
    others = [place + heads * ((group + j) % groups) for j in range(1, groups)]
    weight_copy = pltpu.make_async_copy(weight_hbm, weight_ref, weight_sem)
    weight_copy.start()
    enter([sibling] + neighbours + others)
    own_rows = pl.ds(pl.multiple_of(group * group_rows, group_rows), group_rows)
    copies = []
    arriving = []
    for j in range(1, groups):
        for source, target, send, recv in (
            (gated_ref, all_gated.at[own_rows], gated_send, gated_recv),
            (scaling_ref, all_scaling.at[group], scaling_send, scaling_recv),
        ):
            copy = remote(source, target, send.at[j - 1], recv.at[j - 1], others[j - 1])
            copy.start()
            copies.append(copy)
    all_gated[own_rows, :] = gated_ref[...]
    all_scaling[group] = scaling_ref[...]
    for copy in copies:
        copy.wait_recv()
    weight_copy.wait()
    wide = max(group_rows, 128)
    for g in range(groups):
        flat = all_scaling[g].astype(jnp.float32)
        if wide > group_rows:
            flat = jnp.concatenate(
                [flat, jnp.zeros((SMALL, wide - group_rows), jnp.float32)], axis=1
            )
        flat = jnp.concatenate([flat, jnp.zeros((128 - SMALL, wide), jnp.float32)], axis=0)
        columns[g * group_rows : (g + 1) * group_rows, :] = flat.T[0:group_rows]

    def relative(owner, mask):
        bits = tuple(bit for bit in range(1, dims + 1) if mask >> (bit - 1) & 1)
        begin = flip(owner, bits) * rows
        return pl.ds(pl.multiple_of(begin, rows), rows)

    def head_rows(owner, masks):
        picks = [relative(owner, mask) for mask in masks]
        left = jnp.concatenate([all_gated[pick, :] for pick in picks], axis=0)
        scale = jnp.concatenate([columns[pick, 0:1] for pick in picks], axis=0)
        product = lax.dot_general(
            left, weight_ref[...], (((1,), (1,)), ((), ())), preferred_element_type=jnp.float32
        )
        return product * scale

    core_copies = [
        remote(
            core_out.at[mask], core_in.at[mask], core_send.at[mask], core_recv.at[mask], sibling
        )
        for mask in range(chips)
    ]
    batch_of = min(4, chips)
    sweep = list(range(chips - 1, -1, -1))
    for first in range(0, chips, batch_of):
        masks = sweep[first : first + batch_of]
        product = head_rows(flip(place, (0,)), masks).astype(jnp.bfloat16)
        for i, mask in enumerate(masks):
            core_out[mask] = product[i * rows : (i + 1) * rows]
            core_copies[mask].start()
    for first in range(0, chips, batch_of):
        masks = sweep[first : first + batch_of]
        product = head_rows(place, masks)
        for i, mask in enumerate(masks):
            held[mask] = product[i * rows : (i + 1) * rows]

    parts = parts_of(cols, dims)
    hops = []
    waiting = [[] for _ in range(dims)]

    def cross(step, p, mask):
        (start, width), order = parts[p]
        if step == dims or not mask >> (order[step] - 1) & 1:
            return
        span = pl.ds(start, width)
        landed = mask - (1 << (order[step] - 1))
        hop_out[step, landed, :, span] = held[mask, :, span].astype(jnp.bfloat16)
        copy = remote(
            hop_out.at[step, landed, :, span],
            hop_in.at[step, landed, :, span],
            hop_send.at[step, p, landed],
            hop_recv.at[step, p, landed],
            neighbours[order[step] - 1],
        )
        copy.start()
        hops.append(copy)
        waiting[step].append((p, landed, span, copy))

    for mask in sweep:
        core_copies[mask].wait_recv()
        held[mask] += core_in[mask].astype(jnp.float32)
        for p in range(len(parts)):
            cross(0, p, mask)
    for step in range(dims):
        for p, landed, span, copy in waiting[step]:
            copy.wait_recv()
            held[landed, :, span] += hop_in[step, landed, :, span].astype(jnp.float32)
            cross(step + 1, p, landed)
    out_ref[...] = (stream_ref[...].astype(jnp.float32) + held[0]).astype(jnp.bfloat16)
    for copy in copies + core_copies + hops:
        copy.wait_send()


def output(stream, gated, scaling, out_weight, heads, groups):
    rows, cols = stream.shape
    batch = rows * heads
    group_rows, size = gated.shape
    dims = heads.bit_length() - 2
    chips = 1 << dims
    parts = len(parts_of(cols, dims))
    extra = groups - 1
    dma = pltpu.SemaphoreType.DMA
    anywhere = pl.BlockSpec(memory_space=pl.ANY)
    return pl.pallas_call(
        functools.partial(output_kernel, heads, groups),
        in_specs=[VMEM] * 3 + [anywhere],
        out_specs=VMEM,
        out_shape=jax.ShapeDtypeStruct(stream.shape, stream.dtype),
        scratch_shapes=[
            pltpu.VMEM(out_weight.shape, out_weight.dtype),
            dma(()),
            pltpu.VMEM((batch, size), jnp.bfloat16),
            pltpu.VMEM((groups, SMALL, group_rows), jnp.bfloat16),
            pltpu.VMEM((batch, 128), jnp.float32),
            pltpu.VMEM((chips, rows, cols), jnp.float32),
            pltpu.VMEM((chips, rows, cols), jnp.bfloat16),
            pltpu.VMEM((chips, rows, cols), jnp.bfloat16),
            pltpu.VMEM((dims, chips, rows, cols), jnp.bfloat16),
            pltpu.VMEM((dims, chips, rows, cols), jnp.bfloat16),
            dma((extra,)),
            dma((extra,)),
            dma((extra,)),
            dma((extra,)),
            dma((chips,)),
            dma((chips,)),
            dma((dims, parts, chips)),
            dma((dims, parts, chips)),
        ],
        compiler_params=pltpu.CompilerParams(
            collective_id=1, has_side_effects=True
        ),
    )(stream, gated, scaling, out_weight)


def per_device(
    stream,
    norm_gain,
    query_weight,
    key_weight,
    value_weight,
    gate_weight,
    write_weight,
    decay_weight,
    decay_rate,
    head_gain,
    out_weight,
    state,
):
    heads = decay_rate.shape[0]
    groups = lax.axis_size("tp") // heads
    weights = (query_weight, key_weight, value_weight, gate_weight)
    packed = project(
        stream, norm_gain, weights, write_weight, decay_weight, decay_rate, heads, groups
    )
    updated, gated, scaling = state_step(state, packed, head_gain)
    result = output(stream, gated, scaling, out_weight, heads, groups)
    return (result, updated)


def solution(mesh):
    placed = (
        P("tp", None),
        P(),
        P("tp", None),
        P("tp", None),
        P("tp", None),
        P("tp", None),
        P(),
        P(),
        P(),
        P(),
        P("tp", None),
        P("tp", None, None),
    )
    return jax.shard_map(
        per_device,
        mesh=mesh,
        in_specs=placed,
        out_specs=(P("tp", None), P("tp", None, None)),
        check_vma=False,
    )
```
